32 devices in a mesh: kv: 8 (over z, y), tp: 4 (over x, core).
Axes of the slice: x: 2, y: 2, z: 4, core: 2. Of those that a mesh axis runs over, the one named last changes fastest.
Arguments:
- inputs: bfloat16 [256, 4096], P(None, 'kv'), may hold values from -150 to 150
- norm_gain: bfloat16 [4096], P('kv'), may hold values from 0.099609375 to 1.8984375
- w_query: bfloat16 [4096, 2048], P('kv', 'tp'), may hold values from -0.09375 to 0.09375
- w_forget: bfloat16 [4096, 2048], P('kv', 'tp'), may hold values from -0.09375 to 0.09375
- w_value: bfloat16 [4096, 2048], P('kv', 'tp'), may hold values from -0.09375 to 0.09375
- lower_bound: float32 [2048], P('tp'), may hold values from 0.05 to 0.9
- head_gain: float32 [2048], P('tp'), may hold values from 0.1 to 1.9
- w_out: bfloat16 [2048, 4096], P('tp', 'kv'), may hold values from -0.125 to 0.125
- prior_state: float32 [64, 16, 128, 128], P('kv', 'tp'), may hold values from -3 to 3
- prev_forget: float32 [64, 4, 2048], P('kv', None, 'tp'), may hold values from 0.3 to 0.97
- prev_values: bfloat16 [64, 4, 2048], P('kv', None, 'tp'), may hold values from -6 to 6
- accepted: int32 [64], P('kv'), may hold values from 0 to 4
Outputs:
- mixed_out: bfloat16 [256, 4096], P(None, ('kv', 'tp'))
- base_state: float32 [64, 16, 128, 128], P('kv', 'tp')
The draws below stay inside these ranges and needn't reach their ends.
All inputs are finite; a program needn't handle non-finite values.
Results may differ from the reference program's by a relative error of at most 0.01.
Values may be sent and summed in bfloat16 or wider, within the bound.
No kernel may reach another device: no remote copies, remote signals or barrier semaphores. Data moves between devices by JAX's collectives and lax.ppermute only.
A program may use at most 64 MiB of HBM per device.

```python
import jax
import jax.numpy as jnp
from jax import lax

D = 4096
HEADS = 16
HEAD_SIZE = 128
PROPOSALS = 4
HEAD_WIDTH = 2048
SEQS = 64
TOKENS = 256
N_TP = 4


def draw_inputs(key, part):
    split_keys = jax.random.split(key, 4)
    column = jnp.arange(D, dtype=jnp.float32)[None, :] / D
    row_scale = 10.0 ** jax.random.uniform(split_keys[0], (TOKENS, 1), jnp.float32) / 3.0
    entries = jnp.clip(jax.random.normal(split_keys[1], (TOKENS, D), jnp.float32), -4.0, 4.0)
    column_scale = 10.0 ** (1.6 * column + 0.2 * jax.random.uniform(split_keys[3], (1, D), jnp.float32) - 0.9)
    return (entries * row_scale * column_scale).astype(jnp.bfloat16)


def set_ends(drawn, stream_key, smallest, largest):
    spot = [jax.random.randint(jax.random.fold_in(stream_key, axis), (), 0, length) for axis, length in enumerate(drawn.shape)]
    widest = drawn.shape.index(max(drawn.shape))
    beside = spot[:widest] + [(spot[widest] + 1) % drawn.shape[widest]] + spot[widest + 1:]
    return drawn.at[tuple(spot)].set(smallest).at[tuple(beside)].set(largest)


def shard_levels(rng, extent, pieces, low, high):
    factor_of = 1.0
    for dim, shards_of in pieces:
        draws = jax.random.uniform(jax.random.fold_in(jax.random.fold_in(rng, 6), dim), (shards_of,), jnp.float32, low / len(pieces), high / len(pieces))
        factor_of = factor_of * jnp.repeat(jnp.exp(draws), extent[dim] // shards_of).reshape((-1,) + (1,) * (len(extent) - 1 - dim))
    return factor_of


def normal_values(rng, extent, scale, reach, cuts=(), kind=jnp.bfloat16):
    result = scale * jax.random.normal(rng, extent, jnp.float32)
    if cuts:
        result = result * shard_levels(rng, extent, cuts, -0.22, 0.18)
    return jnp.clip(result, -reach, reach).astype(kind)


def setup_inputs(seed: int = 0) -> dict:
    seeds = jax.random.split(jax.random.key(seed), 13)
    return {
        "inputs": draw_inputs(jax.random.fold_in(seeds[12], 71), 0),
        "norm_gain": jnp.clip(1.0 + 0.18 * jax.random.normal(seeds[1], (D,), jnp.float32), 0.099609375, 1.8984375).astype(jnp.bfloat16),
        "w_query": normal_values(seeds[2], (D, HEAD_WIDTH), D ** -0.5, 0.09375, ((0, 8), (1, 4))),
        "w_forget": normal_values(seeds[3], (D, HEAD_WIDTH), D ** -0.5, 0.09375, ((0, 8), (1, 4))),
        "w_value": normal_values(seeds[4], (D, HEAD_WIDTH), D ** -0.5, 0.09375, ((0, 8), (1, 4))),
        "lower_bound": jnp.clip(0.05 + 0.84999998 * jax.random.uniform(seeds[5], (HEAD_WIDTH,), jnp.float32) ** shard_levels(seeds[5], (HEAD_WIDTH,), ((0, 4),), -0.2, 0.2), 0.05, 0.9),
        "head_gain": jnp.clip(1.0 + 0.18 * jax.random.normal(seeds[6], (HEAD_WIDTH,), jnp.float32), 0.1, 1.9),
        "w_out": normal_values(seeds[7], (HEAD_WIDTH, D), HEAD_WIDTH ** -0.5, 0.125, ((0, 4), (1, 8))),
        "prior_state": normal_values(seeds[8], (SEQS, HEADS, HEAD_SIZE, HEAD_SIZE), 0.5, 3.0, ((0, 8), (1, 4)), jnp.float32),
        "prev_forget": jnp.clip(0.3 + 0.67 * jax.random.uniform(seeds[9], (SEQS, PROPOSALS, HEAD_WIDTH), jnp.float32) ** shard_levels(seeds[9], (SEQS, PROPOSALS, HEAD_WIDTH), ((0, 8), (2, 4)), -0.2, 0.2), 0.3, 0.97),
        "prev_values": normal_values(seeds[10], (SEQS, PROPOSALS, HEAD_WIDTH), 1.0, 6.0, ((0, 8), (2, 4))),
        "accepted": set_ends(jax.random.randint(seeds[11], (SEQS,), 0, PROPOSALS + 1), jax.random.fold_in(seeds[11], 1), 0, PROPOSALS).astype(jnp.int32),
    }


EPSILON = 1e-06

def recurrence(query_pre, forget_pre, value_pre, lower_bound, head_gain, prior_state, prev_forget, prev_values, accepted):
    sequences = prior_state.shape[0]
    heads = prior_state.shape[1]
    head_size = prior_state.shape[2]
    proposals = prev_forget.shape[1]
    layout = (sequences, proposals, heads, head_size)
    floor_gate = lower_bound.reshape(heads, head_size)
    forget_gate = floor_gate + (1.0 - floor_gate) * jax.nn.sigmoid(forget_pre.reshape(layout))
    keys_new = 1.0 - forget_gate
    queries = jax.nn.silu(query_pre.reshape(layout))
    values = value_pre.reshape(layout)
    old_gate = prev_forget.reshape(layout)
    old_values = prev_values.astype(jnp.float32).reshape(layout)
    carried = prior_state
    for position in range(proposals):
        folded = old_gate[:, position, :, :, None] * carried + (1.0 - old_gate[:, position])[..., None] * old_values[:, position, :, None, :]
        taken_up = (position < accepted)[:, None, None, None]
        carried = jnp.where(taken_up, folded, carried)
    base_state = carried
    results = []
    for position in range(proposals):
        carried = forget_gate[:, position, :, :, None] * carried + keys_new[:, position, :, :, None] * values[:, position, :, None, :]
        results.append(jnp.einsum('shk,shkv->shv', queries[:, position], carried, precision=lax.Precision.HIGHEST))
    stacked = jnp.stack(results, axis=1)
    inverse_rms = lax.rsqrt(lax.optimization_barrier(jnp.mean(stacked * stacked, axis=-1, keepdims=True)) + EPSILON)
    normed = stacked * inverse_rms * head_gain.reshape(heads, head_size)
    return (normed.astype(jnp.bfloat16).reshape(sequences * proposals, heads * head_size), base_state)

def project(scaled, weight, rscale):
    return jnp.dot(scaled, weight, preferred_element_type=jnp.float32) * rscale[:, None]

def reference(inputs, norm_gain, w_query, w_forget, w_value, lower_bound, head_gain, w_out, prior_state, prev_forget, prev_values, accepted):
    widened = inputs.astype(jnp.float32)
    squares = lax.optimization_barrier(jnp.sum(widened * widened, axis=1))
    rscale = lax.rsqrt(squares / D + EPSILON)
    scaled = (widened * norm_gain.astype(jnp.float32)).astype(jnp.bfloat16)
    query_pre = project(scaled, w_query, rscale)
    forget_pre = project(scaled, w_forget, rscale)
    value_pre = project(scaled, w_value, rscale)
    normed, base_state = recurrence(query_pre, forget_pre, value_pre, lower_bound, head_gain, prior_state, prev_forget, prev_values, accepted)
    span_width = HEAD_WIDTH // N_TP
    mixed_out = jnp.zeros((TOKENS, D), jnp.float32)
    for member in range(N_TP):
        partial_value = jnp.dot(normed[:, member * span_width:(member + 1) * span_width], w_out[member * span_width:(member + 1) * span_width], preferred_element_type=jnp.float32)
        rounded = lax.optimization_barrier(partial_value.astype(jnp.bfloat16))
        mixed_out = mixed_out + rounded.astype(jnp.float32)
    return (mixed_out.astype(jnp.bfloat16), base_state)
```

```python
import functools

import jax
import jax.numpy as jnp
from jax import lax
from jax.experimental import pallas as pl
from jax.experimental.pallas import tpu as pltpu
from jax.sharding import PartitionSpec as P

EPSILON = 1e-06
LANES = 128
PACK = 16


f32 = jnp.float32
bf16 = jnp.bfloat16
VMEM = pltpu.VMEM


def round_up(n, m):
    return -(-n // m) * m


def split(x):
    high = x.astype(bf16)
    return high, (x - high.astype(f32)).astype(bf16)


def project_kernel(parts, x_hbm, gain_ref, wq_hbm, wf_hbm, wv_hbm, *rest):
    outs = rest[:parts]
    x_ref, w_ref, terms_ref, sems = rest[parts:]
    tokens, features = x_ref.shape
    cols = wq_hbm.shape[1]
    local = tokens // parts
    copies = [pltpu.make_async_copy(x_hbm, x_ref, sems.at[0])]
    for j, w in enumerate((wq_hbm, wf_hbm, wv_hbm)):
        copies.append(pltpu.make_async_copy(w, w_ref.at[j], sems.at[1 + j]))
    for c in copies:
        c.start()
    copies[0].wait()
    wide = x_ref[...].astype(f32)
    scaled = (wide * gain_ref[...].astype(f32)).astype(bf16)
    squares = wide * wide
    folded = squares[:, :LANES]
    for b in range(1, features // LANES):
        folded = folded + squares[:, b * LANES : (b + 1) * LANES]
    row = jnp.sum(folded.T, axis=0, keepdims=True)
    rows = round_up(tokens, LANES) // LANES
    spread = jnp.concatenate(
        [row[:, r * LANES : (r + 1) * LANES] for r in range(rows)], axis=0
    )
    high = spread.astype(bf16).astype(f32)
    extra = jnp.concatenate((high, spread - high), axis=0)
    pad = round_up(2 * rows, PACK) - 2 * rows
    if pad:
        extra = jnp.concatenate((extra, jnp.zeros((pad, LANES), f32)), axis=0)
    extra = extra.astype(bf16)
    for j in range(3):
        copies[1 + j].wait()
        terms = jnp.dot(scaled, w_ref[j], preferred_element_type=f32)
        terms_ref[:, j * cols : (j + 1) * cols] = terms.astype(bf16)
    me = lax.axis_index("kv")
    blocks = 3 * cols // LANES
    for k in range(parts):
        dest = lax.rem(me + k, parts)
        piece = terms_ref[pl.ds(pl.multiple_of(dest * local, PACK), local), :]
        for b in range(blocks):
            outs[k][b * local : (b + 1) * local, :] = piece[:, b * LANES : (b + 1) * LANES]
        outs[k][blocks * local :, :] = extra


def project(inputs, norm_gain, w_query, w_forget, w_value, parts):
    tokens, features = inputs.shape
    cols = w_query.shape[1]
    local = tokens // parts
    height = 3 * cols // LANES * local + round_up(2 * round_up(tokens, LANES) // LANES, PACK)
    anywhere = pl.BlockSpec(memory_space=pl.ANY)
    whole = pl.BlockSpec(memory_space=VMEM)
    return pl.pallas_call(
        functools.partial(project_kernel, parts),
        out_shape=[jax.ShapeDtypeStruct((height, LANES), bf16)] * parts,
        in_specs=[anywhere, whole, anywhere, anywhere, anywhere],
        out_specs=[whole] * parts,
        scratch_shapes=[
            VMEM((tokens, features), bf16),
            VMEM((3, features, cols), bf16),
            VMEM((tokens, 3 * cols), bf16),
            pltpu.SemaphoreType.DMA((4,)),
        ],
        name="project",
    )(inputs, norm_gain.reshape(1, features), w_query, w_forget, w_value)


def fold_kernel(accepted_ref, after_ref, state_ref, gate_ref, value_ref, base_ref, high_ref, low_ref):
    del after_ref
    heads, size, _ = state_ref.shape[1:]
    proposals = gate_ref.shape[1]
    taken = accepted_ref[pl.program_id(0)]
    gates = gate_ref[0]
    values = value_ref[0]
    total = jnp.ones_like(gates[:1])
    weights = [None] * proposals
    for j in reversed(range(proposals)):
        use = j < taken
        gate = gates[j : j + 1]
        weights[j] = jnp.where(use, (1.0 - gate) * total, 0.0)
        total = jnp.where(use, gate * total, total)
    weights = jnp.concatenate(weights, axis=0)
    w1 = weights.astype(bf16)
    rest = weights - w1.astype(f32)
    w2 = rest.astype(bf16)
    w3 = (rest - w2.astype(f32)).astype(bf16)
    stacked = jnp.concatenate((w1, w2, w3), axis=0)
    tripled = jnp.concatenate((values, values, values), axis=0)
    for h in range(heads):
        at = slice(h * size, (h + 1) * size)
        update = lax.dot_general(
            stacked[:, at], tripled[:, at], (((0,), (0,)), ((), ())), preferred_element_type=f32
        )
        column = jnp.broadcast_to(total[:, at], (size, size)).T
        base = column * state_ref[0, h] + update
        base_ref[0, h] = base
        high, low = split(base)
        high_ref[0, h] = high
        low_ref[0, h] = low


def fold(accepted, after, prior_state, prev_forget, prev_values):
    seqs, heads, size, _ = prior_state.shape
    proposals, cols = prev_forget.shape[1:]
    block = pl.BlockSpec((1, heads, size, size), lambda s: (s, 0, 0, 0))
    rows = pl.BlockSpec((1, proposals, cols), lambda s: (s, 0, 0))
    return pl.pallas_call(
        fold_kernel,
        grid=(seqs,),
        out_shape=[
            jax.ShapeDtypeStruct(prior_state.shape, f32),
            jax.ShapeDtypeStruct(prior_state.shape, bf16),
            jax.ShapeDtypeStruct(prior_state.shape, bf16),
        ],
        in_specs=[
            pl.BlockSpec(memory_space=pltpu.SMEM),
            pl.BlockSpec(memory_space=pl.ANY),
            block,
            rows,
            rows,
        ],
        out_specs=[block] * 3,
        cost_estimate=pl.CostEstimate(
            flops=2_000_000_000, bytes_accessed=12 * prior_state.size, transcendentals=0
        ),
        name="fold",
    )(accepted, after, prior_state, prev_forget, prev_values)


def recur_kernel(parts, seqs, proposals, width, *refs):
    pieces = refs[:parts]
    floor_ref, gain_ref, high_ref, low_ref, out_ref, sum_ref, rows_ref = refs[parts:]
    heads, size = high_ref.shape[1], high_ref.shape[2]
    local = seqs * proposals
    tokens = local * parts
    total = pieces[0][...].astype(f32)
    for p in pieces[1:]:
        total = total + p[...].astype(f32)
    used = 3 * heads * local
    me = lax.axis_index("kv")
    rows = round_up(tokens, LANES) // LANES
    squares = total[used : used + rows] + total[used + rows : used + 2 * rows]
    lane = lax.broadcasted_iota(jnp.int32, (local, LANES), 1)
    token = lax.broadcasted_iota(jnp.int32, (local, LANES), 0) + me * local
    picked = jnp.zeros((local, LANES), f32)
    for r in range(rows):
        picked = jnp.where(lane + r * LANES == token, squares[r : r + 1], picked)
    column = jnp.sum(picked, axis=1, keepdims=True)
    scale = lax.rsqrt(column / width + EPSILON)
    for b in range(3 * heads):
        sum_ref[b * local : (b + 1) * local, :] = total[b * local : (b + 1) * local] * scale
    for h in range(heads):
        at = slice(h * size, (h + 1) * size)

        def take(kind, t):
            return sum_ref[pl.ds((kind * heads + h) * local + t, seqs, stride=proposals), :]

        floor = floor_ref[:, at]
        head_gain = gain_ref[:, at]
        query, forget, key, value = [], [], [], []
        for t in range(proposals):
            q = take(0, t)
            query.append(q / (1.0 + jnp.exp(-q)))
            g = floor + (1.0 - floor) / (1.0 + jnp.exp(-take(1, t)))
            forget.append(g)
            key.append(1.0 - g)
            value.append(take(2, t))
        lefts = []
        mixes = []
        for t in range(proposals):
            carried = query[t]
            mix = None
            for j in reversed(range(t + 1)):
                weight = jnp.sum(carried * key[j], axis=1, keepdims=True) * value[j]
                mix = weight if mix is None else mix + weight
                carried = carried * forget[j]
            lefts.append(carried)
            mixes.append(mix)
        highs = [x.astype(bf16).astype(f32) for x in lefts]
        lows = [x - y for x, y in zip(lefts, highs)]
        both = jnp.concatenate(highs + lows, axis=0)
        sub_all = lax.broadcasted_iota(jnp.int32, both.shape, 0) % seqs
        left = jnp.concatenate(
            [jnp.where(sub_all == s, both, 0.0).astype(bf16) for s in range(seqs)], axis=1
        )
        high = high_ref[:, h].reshape(seqs * size, size)
        low = low_ref[:, h].reshape(seqs * size, size)
        first = jnp.dot(left, high, preferred_element_type=f32)
        second = jnp.dot(left[:local], low, preferred_element_type=f32)
        read = first[:local] + first[local:] + second
        for t in range(proposals):
            result = read[t * seqs : (t + 1) * seqs] + mixes[t]
            mean = jnp.sum(result * result, axis=1, keepdims=True) / size
            rows_ref[pl.ds(h * local + t, seqs, stride=proposals), :] = (
                result * lax.rsqrt(mean + EPSILON) * head_gain
            )
        out_ref[:, at] = rows_ref[h * local : (h + 1) * local, :].astype(bf16)


def recur(pieces, lower_bound, head_gain, high, low, proposals, width):
    parts = len(pieces)
    seqs, heads, size, _ = high.shape
    local = seqs * proposals
    cols = heads * size
    whole = pl.BlockSpec(memory_space=VMEM)
    return pl.pallas_call(
        functools.partial(recur_kernel, parts, seqs, proposals, width),
        out_shape=jax.ShapeDtypeStruct((local, cols), bf16),
        in_specs=[whole] * (parts + 4),
        out_specs=whole,
        scratch_shapes=[VMEM((3 * heads * local, size), f32), VMEM((heads * local, size), f32)],
        name="recur",
    )(*pieces, lower_bound.reshape(1, cols), head_gain.reshape(1, cols), high, low)


def mix_kernel(parts, groups, *refs):
    pieces = refs[:parts]
    w_ref = refs[parts]
    outs = refs[parts + 1 : parts + 1 + groups]
    rows_ref, cols_ref = refs[parts + 1 + groups :]
    local = pieces[0].shape[0]
    me = lax.axis_index("kv")
    for k in range(parts):
        source = lax.rem(me + (parts - k), parts)
        rows_ref[pl.ds(pl.multiple_of(source * local, PACK), local), :] = pieces[k][...]
    partial = jnp.dot(rows_ref[...], w_ref[...], preferred_element_type=f32).astype(bf16)
    span = partial.shape[1] // groups
    for g in range(groups):
        cols_ref[g] = partial[:, g * span : (g + 1) * span]
    mine = lax.axis_index("tp")
    for k in range(groups):
        outs[k][...] = cols_ref[lax.rem(mine + k, groups)]


def mix(pieces, w_out, groups):
    parts = len(pieces)
    local, depth = pieces[0].shape
    cols = w_out.shape[1]
    whole = pl.BlockSpec(memory_space=VMEM)
    shape = jax.ShapeDtypeStruct((parts * local, cols // groups), bf16)
    return pl.pallas_call(
        functools.partial(mix_kernel, parts, groups),
        out_shape=[shape] * groups,
        in_specs=[whole] * (parts + 1),
        out_specs=[whole] * groups,
        scratch_shapes=[
            VMEM((parts * local, depth), bf16),
            VMEM((groups, parts * local, cols // groups), bf16),
        ],
        name="mix",
    )(*pieces, w_out)


def far_first(parts):
    return sorted(range(1, parts), key=lambda k: -min(k, parts - k))


def shift(x, axis, k, n):
    return lax.ppermute(x, axis, [(s, (s + k) % n) for s in range(n)])


def body(
    parts,
    groups,
    inputs,
    norm_gain,
    w_query,
    w_forget,
    w_value,
    lower_bound,
    head_gain,
    w_out,
    prior_state,
    prev_forget,
    prev_values,
    accepted,
):
    width = inputs.shape[1] * parts
    terms = project(inputs, norm_gain, w_query, w_forget, w_value, parts)
    arrived = [terms[0]] + [None] * (parts - 1)
    for k in far_first(parts):
        arrived[k] = shift(terms[k], "kv", k, parts)
    base_state, high, low = fold(accepted, terms[0], prior_state, prev_forget, prev_values)
    normed = recur(arrived, lower_bound, head_gain, high, low, prev_forget.shape[1], width)
    gathered = [normed] + [None] * (parts - 1)
    for k in far_first(parts):
        gathered[k] = shift(normed, "kv", k, parts)
    partials = mix(gathered, w_out, groups)
    total = partials[0].astype(f32)
    for k in far_first(groups):
        total = total + shift(partials[k], "tp", k, groups).astype(f32)
    return total.astype(bf16), base_state


def solution(mesh):
    in_specs = (
        P(None, "kv"),
        P("kv"),
        P("kv", "tp"),
        P("kv", "tp"),
        P("kv", "tp"),
        P("tp"),
        P("tp"),
        P("tp", "kv"),
        P("kv", "tp", None, None),
        P("kv", None, "tp"),
        P("kv", None, "tp"),
        P("kv"),
    )
    out_specs = (P(None, ("kv", "tp")), P("kv", "tp", None, None))
    step = functools.partial(body, mesh.shape["kv"], mesh.shape["tp"])
    return jax.shard_map(step, mesh=mesh, in_specs=in_specs, out_specs=out_specs, check_vma=False)
```

```python
import functools

import jax
import jax.numpy as jnp
from jax import lax
from jax.experimental import pallas as pl
from jax.experimental.pallas import tpu as pltpu
from jax.sharding import PartitionSpec as P

EPSILON = 1e-06
LANES = 128
PACK = 16


f32 = jnp.float32
bf16 = jnp.bfloat16
VMEM = pltpu.VMEM


def grant(mib):
    return pltpu.CompilerParams(vmem_limit_bytes=mib << 20)


def in_hbm(*arrays):
    return [pltpu.with_memory_space_constraint(a, pltpu.HBM) for a in arrays]


def round_up(n, m):
    return -(-n // m) * m


def split(x):
    high = x.astype(bf16)
    return high, (x - high.astype(f32)).astype(bf16)


def project_kernel(parts, x_hbm, gain_hbm, wq_hbm, wf_hbm, wv_hbm, *rest):
    outs = rest[:parts]
    x_ref, gain_ref, w_ref, terms_ref, sems = rest[parts:]
    tokens, features = x_ref.shape
    cols = wq_hbm.shape[1]
    local = tokens // parts
    copies = [
        pltpu.make_async_copy(x_hbm, x_ref, sems.at[0]),
        pltpu.make_async_copy(gain_hbm, gain_ref, sems.at[1]),
    ]
    for j, w in enumerate((wq_hbm, wf_hbm, wv_hbm)):
        copies.append(pltpu.make_async_copy(w, w_ref.at[j], sems.at[2 + j]))
    for c in copies:
        c.start()
    copies[0].wait()
    copies[1].wait()
    wide = x_ref[...].astype(f32)
    scaled = (wide * gain_ref[...].astype(f32).reshape(1, features)).astype(bf16)
    squares = wide * wide
    folded = squares[:, :LANES]
    for b in range(1, features // LANES):
        folded = folded + squares[:, b * LANES : (b + 1) * LANES]
    row = jnp.sum(folded.T, axis=0, keepdims=True)
    rows = round_up(tokens, LANES) // LANES
    spread = jnp.concatenate(
        [row[:, r * LANES : (r + 1) * LANES] for r in range(rows)], axis=0
    )
    high = spread.astype(bf16).astype(f32)
    extra = jnp.concatenate((high, spread - high), axis=0)
    pad = round_up(2 * rows, PACK) - 2 * rows
    if pad:
        extra = jnp.concatenate((extra, jnp.zeros((pad, LANES), f32)), axis=0)
    extra = extra.astype(bf16)
    for j in range(3):
        copies[2 + j].wait()
        terms = jnp.dot(scaled, w_ref[j], preferred_element_type=f32)
        terms_ref[:, j * cols : (j + 1) * cols] = terms.astype(bf16)
    me = lax.axis_index("kv")
    blocks = 3 * cols // LANES
    for k in range(parts):
        dest = lax.rem(me + k, parts)
        piece = terms_ref[pl.ds(pl.multiple_of(dest * local, PACK), local), :]
        for b in range(blocks):
            outs[k][b * local : (b + 1) * local, :] = piece[:, b * LANES : (b + 1) * LANES]
        outs[k][blocks * local :, :] = extra


def project(inputs, norm_gain, w_query, w_forget, w_value, parts):
    tokens, features = inputs.shape
    cols = w_query.shape[1]
    local = tokens // parts
    height = 3 * cols // LANES * local + round_up(2 * round_up(tokens, LANES) // LANES, PACK)
    anywhere = pl.BlockSpec(memory_space=pltpu.HBM)
    whole = pl.BlockSpec(memory_space=VMEM)
    return pl.pallas_call(
        functools.partial(project_kernel, parts),
        out_shape=[jax.ShapeDtypeStruct((height, LANES), bf16)] * parts,
        in_specs=[anywhere] * 5,
        out_specs=[whole] * parts,
        scratch_shapes=[
            VMEM((tokens, features), bf16),
            VMEM((features,), bf16),
            VMEM((3, features, cols), bf16),
            VMEM((tokens, 3 * cols), bf16),
            pltpu.SemaphoreType.DMA((5,)),
        ],
        compiler_params=grant(24),
        name="project",
    )(*in_hbm(inputs, norm_gain, w_query, w_forget, w_value))


def fold_kernel(accepted_ref, after_ref, state_ref, gate_ref, value_ref, base_ref, high_ref, low_ref):
    del after_ref
    heads, size, _ = state_ref.shape[1:]
    proposals = gate_ref.shape[1]
    taken = accepted_ref[pl.program_id(0)]
    gates = gate_ref[0]
    values = value_ref[0].astype(f32)
    total = jnp.ones_like(gates[:1])
    weights = [None] * proposals
    for j in reversed(range(proposals)):
        use = j < taken
        gate = gates[j : j + 1]
        weights[j] = jnp.where(use, (1.0 - gate) * total, 0.0)
        total = jnp.where(use, gate * total, total)
    exact = jnp.concatenate(weights + [total], axis=0)
    first = exact.astype(bf16).astype(f32)
    second = (exact - first).astype(bf16).astype(f32)
    third = exact - first - second
    each = 3 * (proposals + 1)
    depth = round_up(each, PACK)
    pad = [jnp.zeros((depth - each, exact.shape[1]), f32)] if depth > each else []
    left = jnp.concatenate([first, second, third] + pad, axis=0)
    left = jnp.concatenate([left[:, h * size : (h + 1) * size] for h in range(heads)], axis=0)
    left = left.T.astype(bf16)
    none = jnp.zeros((1, size), f32)
    one = jnp.ones((1, size), f32)
    side = jnp.concatenate(([none] * proposals + [one]) * 3 + [none] * (depth - each), axis=0)
    rows = lax.broadcasted_iota(jnp.int32, (heads * depth, 2 * size), 0) // depth
    for h in range(heads):
        mine = values[:, h * size : (h + 1) * size]
        block = jnp.concatenate([mine, none] * 3 + [none] * (depth - each), axis=0)
        block = jnp.concatenate((block, side), axis=1)
        right = jnp.where(rows == h, jnp.concatenate([block] * heads, axis=0), 0.0).astype(bf16)
        both = jnp.dot(left, right, preferred_element_type=f32)
        base = both[:, size:] * state_ref[0, h] + both[:, :size]
        base_ref[0, h] = base
        high, low = split(base)
        high_ref[0, h] = high
        low_ref[0, h] = low


def fold(accepted, after, prior_state, prev_forget, prev_values):
    seqs, heads, size, _ = prior_state.shape
    proposals, cols = prev_forget.shape[1:]
    block = pl.BlockSpec((1, heads, size, size), lambda s: (s, 0, 0, 0))
    rows = pl.BlockSpec((1, proposals, cols), lambda s: (s, 0, 0))
    return pl.pallas_call(
        fold_kernel,
        grid=(seqs,),
        out_shape=[
            jax.ShapeDtypeStruct(prior_state.shape, f32),
            jax.ShapeDtypeStruct(prior_state.shape, bf16),
            jax.ShapeDtypeStruct(prior_state.shape, bf16),
        ],
        in_specs=[
            pl.BlockSpec(memory_space=pltpu.SMEM),
            pl.BlockSpec(memory_space=pl.ANY),
            block,
            rows,
            rows,
        ],
        out_specs=[block] * 3,
        cost_estimate=pl.CostEstimate(
            flops=2_000_000_000, bytes_accessed=12 * prior_state.size, transcendentals=0
        ),
        compiler_params=grant(16),
        name="fold",
    )(*in_hbm(accepted), after, *in_hbm(prior_state, prev_forget, prev_values))


def recur_kernel(parts, seqs, proposals, width, *refs):
    pieces = refs[:parts]
    floor_ref, gain_ref, high_ref, low_ref, out_ref, sum_ref, rows_ref = refs[parts:]
    heads, size = high_ref.shape[1], high_ref.shape[2]
    local = seqs * proposals
    tokens = local * parts
    total = pieces[0][...].astype(f32)
    for p in pieces[1:]:
        total = total + p[...].astype(f32)
    used = 3 * heads * local
    me = lax.axis_index("kv")
    rows = round_up(tokens, LANES) // LANES
    squares = total[used : used + rows] + total[used + rows : used + 2 * rows]
    lane = lax.broadcasted_iota(jnp.int32, (local, LANES), 1)
    token = lax.broadcasted_iota(jnp.int32, (local, LANES), 0) + me * local
    picked = jnp.zeros((local, LANES), f32)
    for r in range(rows):
        picked = jnp.where(lane + r * LANES == token, squares[r : r + 1], picked)
    column = jnp.sum(picked, axis=1, keepdims=True)
    scale = lax.rsqrt(column / width + EPSILON)
    for b in range(3 * heads):
        sum_ref[b * local : (b + 1) * local, :] = total[b * local : (b + 1) * local] * scale
    for h in range(heads):
        at = slice(h * size, (h + 1) * size)

        def take(kind, t):
            return sum_ref[pl.ds((kind * heads + h) * local + t, seqs, stride=proposals), :]

        floor = floor_ref[:, at]
        head_gain = gain_ref[:, at]
        query, forget, key, value = [], [], [], []
        for t in range(proposals):
            q = take(0, t)
            query.append(q / (1.0 + jnp.exp(-q)))
            g = floor + (1.0 - floor) / (1.0 + jnp.exp(-take(1, t)))
            forget.append(g)
            key.append(1.0 - g)
            value.append(take(2, t))
        lefts = []
        mixes = []
        for t in range(proposals):
            carried = query[t]
            mix = None
            for j in reversed(range(t + 1)):
                weight = jnp.sum(carried * key[j], axis=1, keepdims=True) * value[j]
                mix = weight if mix is None else mix + weight
                carried = carried * forget[j]
            lefts.append(carried)
            mixes.append(mix)
        highs = [x.astype(bf16).astype(f32) for x in lefts]
        lows = [x - y for x, y in zip(lefts, highs)]
        both = jnp.concatenate(highs + lows, axis=0)
        sub_all = lax.broadcasted_iota(jnp.int32, both.shape, 0) % seqs
        left = jnp.concatenate(
            [jnp.where(sub_all == s, both, 0.0).astype(bf16) for s in range(seqs)], axis=1
        )
        high = high_ref[:, h].reshape(seqs * size, size)
        low = low_ref[:, h].reshape(seqs * size, size)
        first = jnp.dot(left, high, preferred_element_type=f32)
        second = jnp.dot(left[:local], low, preferred_element_type=f32)
        read = first[:local] + first[local:] + second
        for t in range(proposals):
            result = read[t * seqs : (t + 1) * seqs] + mixes[t]
            mean = jnp.sum(result * result, axis=1, keepdims=True) / size
            rows_ref[pl.ds(h * local + t, seqs, stride=proposals), :] = (
                result * lax.rsqrt(mean + EPSILON) * head_gain
            )
        out_ref[:, at] = rows_ref[h * local : (h + 1) * local, :].astype(bf16)


def recur(pieces, lower_bound, head_gain, high, low, proposals, width):
    parts = len(pieces)
    seqs, heads, size, _ = high.shape
    local = seqs * proposals
    cols = heads * size
    whole = pl.BlockSpec(memory_space=VMEM)
    return pl.pallas_call(
        functools.partial(recur_kernel, parts, seqs, proposals, width),
        out_shape=jax.ShapeDtypeStruct((local, cols), bf16),
        in_specs=[whole] * (parts + 4),
        out_specs=whole,
        scratch_shapes=[VMEM((3 * heads * local, size), f32), VMEM((heads * local, size), f32)],
        compiler_params=grant(16),
        name="recur",
    )(*pieces, lower_bound.reshape(1, cols), head_gain.reshape(1, cols), high, low)


def mix_kernel(parts, groups, *refs):
    pieces = refs[:parts]
    w_ref = refs[parts]
    outs = refs[parts + 1 : parts + 1 + groups]
    rows_ref, cols_ref = refs[parts + 1 + groups :]
    local = pieces[0].shape[0]
    me = lax.axis_index("kv")
    for k in range(parts):
        source = lax.rem(me + (parts - k), parts)
        rows_ref[pl.ds(pl.multiple_of(source * local, PACK), local), :] = pieces[k][...]
    partial = jnp.dot(rows_ref[...], w_ref[...], preferred_element_type=f32).astype(bf16)
    span = partial.shape[1] // groups
    for g in range(groups):
        cols_ref[g] = partial[:, g * span : (g + 1) * span]
    mine = lax.axis_index("tp")
    for k in range(groups):
        outs[k][...] = cols_ref[lax.rem(mine + k, groups)]


def mix(pieces, w_out, groups):
    parts = len(pieces)
    local, depth = pieces[0].shape
    cols = w_out.shape[1]
    whole = pl.BlockSpec(memory_space=VMEM)
    shape = jax.ShapeDtypeStruct((parts * local, cols // groups), bf16)
    return pl.pallas_call(
        functools.partial(mix_kernel, parts, groups),
        out_shape=[shape] * groups,
        in_specs=[whole] * (parts + 1),
        out_specs=[whole] * groups,
        scratch_shapes=[
            VMEM((parts * local, depth), bf16),
            VMEM((groups, parts * local, cols // groups), bf16),
        ],
        compiler_params=grant(16),
        name="mix",
    )(*pieces, w_out)


def far_first(parts):
    return sorted(range(1, parts), key=lambda k: -min(k, parts - k))


def shift(x, axis, k, n):
    return lax.ppermute(x, axis, [(s, (s + k) % n) for s in range(n)])


def body(
    parts,
    groups,
    inputs,
    norm_gain,
    w_query,
    w_forget,
    w_value,
    lower_bound,
    head_gain,
    w_out,
    prior_state,
    prev_forget,
    prev_values,
    accepted,
):
    width = inputs.shape[1] * parts
    terms = project(inputs, norm_gain, w_query, w_forget, w_value, parts)
    arrived = [terms[0]] + [None] * (parts - 1)
    for k in far_first(parts):
        arrived[k] = shift(terms[k], "kv", k, parts)
    base_state, high, low = fold(accepted, terms[0], prior_state, prev_forget, prev_values)
    normed = recur(arrived, lower_bound, head_gain, high, low, prev_forget.shape[1], width)
    gathered = [normed] + [None] * (parts - 1)
    for k in far_first(parts):
        gathered[k] = shift(normed, "kv", k, parts)
    partials = mix(gathered, w_out, groups)
    total = partials[0].astype(f32)
    for k in far_first(groups):
        total = total + shift(partials[k], "tp", k, groups).astype(f32)
    return total.astype(bf16), base_state


def solution(mesh):
    in_specs = (
        P(None, "kv"),
        P("kv"),
        P("kv", "tp"),
        P("kv", "tp"),
        P("kv", "tp"),
        P("tp"),
        P("tp"),
        P("tp", "kv"),
        P("kv", "tp", None, None),
        P("kv", None, "tp"),
        P("kv", None, "tp"),
        P("kv"),
    )
    out_specs = (P(None, ("kv", "tp")), P("kv", "tp", None, None))
    step = functools.partial(body, mesh.shape["kv"], mesh.shape["tp"])
    return jax.shard_map(step, mesh=mesh, in_specs=in_specs, out_specs=out_specs, check_vma=False)
```

```python
import functools

import jax
import jax.numpy as jnp
from jax import lax
from jax.experimental import pallas as pl
from jax.experimental.pallas import tpu as pltpu
from jax.sharding import PartitionSpec as P

EPSILON = 1e-06
LANES = 128
PACK = 16
PAIR = 2
GROUP = 4


f32 = jnp.float32
bf16 = jnp.bfloat16
VMEM = pltpu.VMEM
WHOLE = pl.BlockSpec(memory_space=pltpu.VMEM)


def grant(mib):
    return pltpu.CompilerParams(vmem_limit_bytes=mib << 20)


def in_hbm(*arrays):
    return [pltpu.with_memory_space_constraint(a, pltpu.HBM) for a in arrays]


def round_up(n, m):
    return -(-n // m) * m


def square_rows(tokens):
    return round_up(tokens, LANES) // LANES


def coded_rows(tokens):
    return round_up(2 * square_rows(tokens), PACK)


def coded(spread):
    rows = spread.shape[0]
    high = spread.astype(bf16).astype(f32)
    parts = [high, spread - high]
    pad = round_up(2 * rows, PACK) - 2 * rows
    if pad:
        parts.append(jnp.zeros((pad, LANES), f32))
    return jnp.concatenate(parts, axis=0).astype(bf16)


def decoded(ref, start, rows):
    tile = ref[start : start + round_up(2 * rows, PACK), :].astype(f32)
    return tile[:rows] + tile[rows : 2 * rows]


def split(x):
    high = x.astype(bf16)
    return high, (x - high.astype(f32)).astype(bf16)


def project_kernel(outer, x_hbm, gain_hbm, wq_hbm, wf_hbm, wv_hbm, *rest):
    across_ref, stay_ref, squares_ref, own_ref = rest[:4]
    ahead = rest[4 : 3 + outer]
    x_ref, gain_ref, w_ref, terms_ref, sems = rest[3 + outer :]
    tokens, features = x_ref.shape
    cols = wq_hbm.shape[1]
    blocks = cols // LANES
    local = tokens // (outer * PAIR)
    copies = [
        pltpu.make_async_copy(x_hbm, x_ref, sems.at[0]),
        pltpu.make_async_copy(gain_hbm, gain_ref, sems.at[1]),
    ]
    for j, w in enumerate((wf_hbm, wv_hbm, wq_hbm)):
        copies.append(pltpu.make_async_copy(w, w_ref.at[j], sems.at[2 + j]))
    for c in copies:
        c.start()
    copies[0].wait()
    copies[1].wait()
    wide = x_ref[...].astype(f32)
    scaled = (wide * gain_ref[...].astype(f32).reshape(1, features)).astype(bf16)
    squares = wide * wide
    folded = squares[:, :LANES]
    for b in range(1, features // LANES):
        folded = folded + squares[:, b * LANES : (b + 1) * LANES]
    row = jnp.sum(folded.T, axis=0, keepdims=True)
    rows = square_rows(tokens)
    spread = jnp.concatenate(
        [row[:, r * LANES : (r + 1) * LANES] for r in range(rows)], axis=0
    )
    squares_ref[...] = spread
    across_ref[outer * 2 * blocks * local :, :] = coded(spread)
    for j in range(3):
        copies[2 + j].wait()
        terms = jnp.dot(scaled, w_ref[j], preferred_element_type=f32)
        for b in range(blocks):
            terms_ref[j * blocks + b] = terms[:, b * LANES : (b + 1) * LANES]
    me = lax.axis_index("kv")
    mine = lax.rem(me, PAIR)
    here = me // PAIR
    for k in range(outer):
        there = target(here, k, outer)
        near = pl.ds(pl.multiple_of((there * PAIR + mine) * local, PACK), local)
        far = pl.ds(pl.multiple_of((there * PAIR + 1 - mine) * local, PACK), local)
        for b in range(2 * blocks):
            at = pl.ds((k * 2 * blocks + b) * local, local)
            stay_ref[at, :] = terms_ref[b, near, :]
            across_ref[at, :] = terms_ref[b, far, :].astype(bf16)
        for b in range(blocks):
            for r, which in enumerate((near, far)):
                at = pl.ds((r * blocks + b) * local, local)
                piece = terms_ref[2 * blocks + b, which, :]
                if k:
                    ahead[k - 1][at, :] = piece.astype(bf16)
                else:
                    own_ref[at, :] = piece


def project(inputs, norm_gain, w_query, w_forget, w_value, outer):
    tokens, features = inputs.shape
    cols = w_query.shape[1]
    blocks = cols // LANES
    local = tokens // (outer * PAIR)
    section = 2 * blocks * local
    shapes = [
        jax.ShapeDtypeStruct((outer * section + coded_rows(tokens), LANES), bf16),
        jax.ShapeDtypeStruct((outer * section, LANES), f32),
        jax.ShapeDtypeStruct((square_rows(tokens), LANES), f32),
        jax.ShapeDtypeStruct((section, LANES), f32),
    ] + [jax.ShapeDtypeStruct((section, LANES), bf16)] * (outer - 1)
    out = pl.pallas_call(
        functools.partial(project_kernel, outer),
        out_shape=shapes,
        in_specs=[pl.BlockSpec(memory_space=pltpu.HBM)] * 5,
        out_specs=[WHOLE] * len(shapes),
        scratch_shapes=[
            VMEM((tokens, features), bf16),
            VMEM((features,), bf16),
            VMEM((3, features, cols), bf16),
            VMEM((3 * blocks, tokens, LANES), f32),
            pltpu.SemaphoreType.DMA((5,)),
        ],
        compiler_params=grant(24),
        name="project",
    )(*in_hbm(inputs, norm_gain, w_query, w_forget, w_value))
    return out[0], out[1], out[2], out[3], out[4:]


def combine_kernel(outer, after_ref, *refs):
    del after_ref
    across_ref, stay_ref, squares_ref, own_ref = refs[:4]
    ahead = refs[4 : 3 + outer]
    outs = refs[3 + outer :]
    sends, (pair_ref, kept_ref, total_ref, half_ref) = outs[: outer - 1], outs[outer - 1 :]
    rows = squares_ref.shape[0]
    section = kept_ref.shape[0]
    squares = squares_ref[...] + decoded(across_ref, outer * section, rows)
    total_ref[...] = squares
    tail = coded(squares)
    for k in range(1, outer):
        at = pl.ds(k * section, section)
        sends[k - 1][:section, :] = (stay_ref[at, :] + across_ref[at, :].astype(f32)).astype(bf16)
        sends[k - 1][section:, :] = tail
    kept_ref[...] = stay_ref[:section, :] + across_ref[:section, :].astype(f32)
    total = own_ref[...]
    for p in ahead:
        total = total + p[...].astype(f32)
    split_at = half_ref.shape[0]
    half_ref[...] = total[:split_at]
    pair_ref[...] = total[split_at:].astype(bf16)


def combine(after, across, stay, squares, own, ahead, outer):
    section = own.shape[0]
    rows = squares.shape[0]
    height = section + round_up(2 * rows, PACK)
    shapes = [jax.ShapeDtypeStruct((height, LANES), bf16)] * (outer - 1) + [
        jax.ShapeDtypeStruct((section // PAIR, LANES), bf16),
        jax.ShapeDtypeStruct((section, LANES), f32),
        jax.ShapeDtypeStruct((rows, LANES), f32),
        jax.ShapeDtypeStruct((section // PAIR, LANES), f32),
    ]
    out = pl.pallas_call(
        functools.partial(combine_kernel, outer),
        out_shape=shapes,
        in_specs=[WHOLE] * (outer + 4),
        out_specs=[WHOLE] * len(shapes),
        compiler_params=grant(16),
        name="combine",
    )(after, across, stay, squares, own, *ahead)
    return out[: outer - 1], *out[outer - 1 :]


def fold_kernel(
    accepted_ref, after_ref, state_hbm, gate_hbm, value_hbm, base_ref, high_ref, low_ref, *rest
):
    del after_ref
    state_ref, gate_ref, value_ref, left_ref, sems, gate_sem, value_sem = rest
    seqs, heads, size, _ = state_ref.shape
    proposals = gate_ref.shape[1]
    gate_copy = pltpu.make_async_copy(gate_hbm, gate_ref, gate_sem)
    value_copy = pltpu.make_async_copy(value_hbm, value_ref, value_sem)
    gate_copy.start()
    value_copy.start()
    loads = [
        pltpu.make_async_copy(state_hbm.at[s], state_ref.at[s], sems.at[s]) for s in range(seqs)
    ]
    for c in loads:
        c.start()
    gate_copy.wait()
    value_copy.wait()
    each = 3 * (proposals + 1)
    depth = round_up(each, PACK)
    none = jnp.zeros((1, size), f32)
    one = jnp.ones((1, size), f32)
    fill = [none] * (depth - each)
    side = jnp.concatenate(([none] * proposals + [one]) * 3 + fill, axis=0)
    for s in range(seqs):
        taken = accepted_ref[s]
        gates = gate_ref[s]
        total = jnp.ones_like(gates[:1])
        weights = [None] * proposals
        for j in reversed(range(proposals)):
            use = j < taken
            gate = gates[j : j + 1]
            weights[j] = jnp.where(use, (1.0 - gate) * total, 0.0)
            total = jnp.where(use, gate * total, total)
        exact = jnp.concatenate(weights + [total], axis=0)
        first = exact.astype(bf16).astype(f32)
        second = (exact - first).astype(bf16).astype(f32)
        third = exact - first - second
        pad = [jnp.zeros((depth - each, exact.shape[1]), f32)] if depth > each else []
        left = jnp.concatenate([first, second, third] + pad, axis=0)
        left = jnp.concatenate([left[:, h * size : (h + 1) * size] for h in range(heads)], axis=0)
        left_ref[s] = left.T.astype(bf16)
    rows = lax.broadcasted_iota(jnp.int32, (heads * depth, 2 * size), 0) // depth
    for s in range(seqs):
        if s % GROUP == 0:
            for c in loads[s : s + GROUP]:
                c.wait()
        values = value_ref[s].astype(f32)
        left = left_ref[s]
        for h in range(heads):
            mine = values[:, h * size : (h + 1) * size]
            block = jnp.concatenate([mine, none] * 3 + fill, axis=0)
            block = jnp.concatenate((block, side), axis=1)
            right = jnp.where(rows == h, jnp.concatenate([block] * heads, axis=0), 0.0)
            both = jnp.dot(left, right.astype(bf16), preferred_element_type=f32)
            base = both[:, size:] * state_ref[s, h] + both[:, :size]
            base_ref[s, h] = base
            high, low = split(base)
            high_ref[s, h] = high
            low_ref[s, h] = low


def fold(accepted, after, prior_state, prev_forget, prev_values):
    seqs, heads, size, _ = prior_state.shape
    proposals = prev_forget.shape[1]
    hbm = pl.BlockSpec(memory_space=pltpu.HBM)
    return pl.pallas_call(
        fold_kernel,
        out_shape=[
            jax.ShapeDtypeStruct(prior_state.shape, f32),
            jax.ShapeDtypeStruct(prior_state.shape, bf16),
            jax.ShapeDtypeStruct(prior_state.shape, bf16),
        ],
        in_specs=[pl.BlockSpec(memory_space=pltpu.SMEM), pl.BlockSpec(memory_space=pl.ANY)]
        + [hbm] * 3,
        out_specs=[WHOLE] * 3,
        scratch_shapes=[
            VMEM(prior_state.shape, f32),
            VMEM(prev_forget.shape, f32),
            VMEM(prev_values.shape, bf16),
            VMEM((seqs, size, heads * round_up(3 * (proposals + 1), PACK)), bf16),
            pltpu.SemaphoreType.DMA((seqs,)),
            pltpu.SemaphoreType.DMA,
            pltpu.SemaphoreType.DMA,
        ],
        cost_estimate=pl.CostEstimate(
            flops=2_000_000_000, bytes_accessed=12 * prior_state.size, transcendentals=0
        ),
        compiler_params=grant(16),
        name="fold",
    )(*in_hbm(accepted), after, *in_hbm(prior_state, prev_forget, prev_values))


def store_kernel(after_ref, base_ref, out_hbm, sems):
    del after_ref
    copies = [
        pltpu.make_async_copy(base_ref.at[s], out_hbm.at[s], sems.at[s])
        for s in range(base_ref.shape[0])
    ]
    for c in copies:
        c.start()
    for c in copies:
        c.wait()


def store(after, base):
    return pl.pallas_call(
        store_kernel,
        out_shape=jax.ShapeDtypeStruct(base.shape, base.dtype),
        in_specs=[WHOLE] * 2,
        out_specs=pl.BlockSpec(memory_space=pltpu.HBM),
        scratch_shapes=[pltpu.SemaphoreType.DMA((base.shape[0],))],
        cost_estimate=pl.CostEstimate(
            flops=1_000_000_000, bytes_accessed=8 * base.size, transcendentals=0
        ),
        compiler_params=grant(8),
        name="store",
    )(after, base)


def recur_kernel(seqs, proposals, width, *refs):
    kept_ref, squares_ref, half_ref, other_ref = refs[:4]
    arrived = refs[4:-7]
    floor_ref, gain_ref, high_ref, low_ref, out_ref, sum_ref, rows_ref = refs[-7:]
    heads, size = high_ref.shape[1], high_ref.shape[2]
    local = seqs * proposals
    rows = squares_ref.shape[0]
    section = kept_ref.shape[0]
    total = kept_ref[...]
    squares = squares_ref[...]
    for p in arrived:
        total = total + p[:section, :].astype(f32)
        squares = squares + decoded(p, section, rows)
    first = half_ref[...] + other_ref[...].astype(f32)
    me = lax.axis_index("kv")
    lane = lax.broadcasted_iota(jnp.int32, (local, LANES), 1)
    token = lax.broadcasted_iota(jnp.int32, (local, LANES), 0) + me * local
    picked = jnp.zeros((local, LANES), f32)
    for r in range(rows):
        picked = jnp.where(lane + r * LANES == token, squares[r : r + 1], picked)
    column = jnp.sum(picked, axis=1, keepdims=True)
    scale = lax.rsqrt(column / width + EPSILON)
    for b in range(heads):
        sum_ref[b * local : (b + 1) * local, :] = first[b * local : (b + 1) * local] * scale
    for b in range(2 * heads):
        at = slice((heads + b) * local, (heads + b + 1) * local)
        sum_ref[at, :] = total[b * local : (b + 1) * local] * scale
    for h in range(heads):
        at = slice(h * size, (h + 1) * size)

        def take(kind, t):
            return sum_ref[pl.ds((kind * heads + h) * local + t, seqs, stride=proposals), :]

        floor = floor_ref[:, at]
        head_gain = gain_ref[:, at]
        query, forget, key, value = [], [], [], []
        for t in range(proposals):
            q = take(0, t)
            query.append(q / (1.0 + jnp.exp(-q)))
            g = floor + (1.0 - floor) / (1.0 + jnp.exp(-take(1, t)))
            forget.append(g)
            key.append(1.0 - g)
            value.append(take(2, t))
        lefts = []
        mixes = []
        for t in range(proposals):
            carried = query[t]
            mix = None
            for j in reversed(range(t + 1)):
                weight = jnp.sum(carried * key[j], axis=1, keepdims=True) * value[j]
                mix = weight if mix is None else mix + weight
                carried = carried * forget[j]
            lefts.append(carried)
            mixes.append(mix)
        highs = [x.astype(bf16).astype(f32) for x in lefts]
        lows = [x - y for x, y in zip(lefts, highs)]
        both = jnp.concatenate(highs + lows, axis=0)
        sub_all = lax.broadcasted_iota(jnp.int32, both.shape, 0) % seqs
        left = jnp.concatenate(
            [jnp.where(sub_all == s, both, 0.0).astype(bf16) for s in range(seqs)], axis=1
        )
        high = high_ref[:, h].reshape(seqs * size, size)
        low = low_ref[:, h].reshape(seqs * size, size)
        first = jnp.dot(left, high, preferred_element_type=f32)
        second = jnp.dot(left[:local], low, preferred_element_type=f32)
        read = first[:local] + first[local:] + second
        for t in range(proposals):
            result = read[t * seqs : (t + 1) * seqs] + mixes[t]
            mean = jnp.sum(result * result, axis=1, keepdims=True) / size
            rows_ref[pl.ds(h * local + t, seqs, stride=proposals), :] = (
                result * lax.rsqrt(mean + EPSILON) * head_gain
            )
        out_ref[:, at] = rows_ref[h * local : (h + 1) * local, :].astype(bf16)


def recur(kept, squares, half, other, arrived, lower_bound, head_gain, high, low, proposals, width):
    seqs, heads, size, _ = high.shape
    local = seqs * proposals
    cols = heads * size
    return pl.pallas_call(
        functools.partial(recur_kernel, seqs, proposals, width),
        out_shape=jax.ShapeDtypeStruct((local, cols), bf16),
        in_specs=[WHOLE] * (len(arrived) + 8),
        out_specs=WHOLE,
        scratch_shapes=[VMEM((3 * heads * local, size), f32), VMEM((heads * local, size), f32)],
        compiler_params=grant(16),
        name="recur",
    )(
        kept,
        squares,
        half,
        other,
        *arrived,
        lower_bound.reshape(1, cols),
        head_gain.reshape(1, cols),
        high,
        low,
    )


def stack_kernel(outer, *refs):
    pieces, out_ref = refs[:outer], refs[outer]
    local = pieces[0].shape[0]
    here = lax.axis_index("kv") // PAIR
    for k in range(outer):
        source = origin(here, k, outer)
        out_ref[pl.ds(pl.multiple_of(source * local, PACK), local), :] = pieces[k][...]


def stack(pieces):
    outer = len(pieces)
    local, cols = pieces[0].shape
    return pl.pallas_call(
        functools.partial(stack_kernel, outer),
        out_shape=jax.ShapeDtypeStruct((outer * local, cols), bf16),
        in_specs=[WHOLE] * outer,
        out_specs=WHOLE,
        compiler_params=grant(8),
        name="stack",
    )(*pieces)


def mix_kernel(outer, groups, *refs):
    near_ref, far_ref, w_ref = refs[:3]
    outs = refs[3 : 3 + groups]
    cols_ref = refs[3 + groups]
    local = near_ref.shape[0] // outer
    span = w_ref.shape[1] // groups
    mine = lax.rem(lax.axis_index("kv"), PAIR)
    for r, ref in enumerate((near_ref, far_ref)):
        partial = jnp.dot(ref[...], w_ref[...], preferred_element_type=f32).astype(bf16)
        side = mine if r == 0 else 1 - mine
        for g in range(groups):
            for z in range(outer):
                at = pl.ds(pl.multiple_of((z * PAIR + side) * local, PACK), local)
                cols_ref[g, at, :] = partial[z * local : (z + 1) * local, g * span : (g + 1) * span]
    me = lax.axis_index("tp")
    for k in range(groups):
        outs[k][...] = cols_ref[target(me, k, groups)]


def mix(near, far, w_out, outer, groups):
    tokens = PAIR * near.shape[0]
    span = w_out.shape[1] // groups
    return pl.pallas_call(
        functools.partial(mix_kernel, outer, groups),
        out_shape=[jax.ShapeDtypeStruct((tokens, span), bf16)] * groups,
        in_specs=[WHOLE] * 3,
        out_specs=[WHOLE] * groups,
        scratch_shapes=[VMEM((groups, tokens, span), bf16)],
        compiler_params=grant(16),
        name="mix",
    )(near, far, w_out)


def target(here, k, count):
    return here ^ k if count & (count - 1) == 0 else (here + k) % count


def origin(here, k, count):
    return here ^ k if count & (count - 1) == 0 else (here + count - k) % count


def far_first(count):
    return sorted(range(1, count), key=lambda k: -k)


def between(x, axis, k, n):
    return lax.ppermute(x, axis, [(s, target(s, k, n)) for s in range(n)])


def swap(x, parts):
    return lax.ppermute(x, "kv", [(s, s - s % PAIR + (s + 1) % PAIR) for s in range(parts)])


def along(x, k, parts):
    count = parts // PAIR
    return lax.ppermute(
        x, "kv", [(s, PAIR * target(s // PAIR, k, count) + s % PAIR) for s in range(parts)]
    )


def body(
    parts,
    groups,
    inputs,
    norm_gain,
    w_query,
    w_forget,
    w_value,
    lower_bound,
    head_gain,
    w_out,
    prior_state,
    prev_forget,
    prev_values,
    accepted,
):
    width = inputs.shape[1] * parts
    outer = parts // PAIR
    order = far_first(outer)
    across, stay, squares, own, ahead = project(
        inputs, norm_gain, w_query, w_forget, w_value, outer
    )
    across = swap(across, parts)
    ahead = [along(ahead[k - 1], k, parts) for k in order]
    base_state, high, low = fold(accepted, stay, prior_state, prev_forget, prev_values)
    sends, pair, kept, squares, half = combine(low, across, stay, squares, own, ahead, outer)
    arrived = [along(sends[k - 1], k, parts) for k in order]
    base_state = store(pair, base_state)
    other = swap(pair, parts)
    normed = recur(
        kept,
        squares,
        half,
        other,
        arrived,
        lower_bound,
        head_gain,
        high,
        low,
        prev_forget.shape[1],
        width,
    )
    column = [normed] + [None] * (outer - 1)
    for k in order:
        column[k] = along(normed, k, parts)
    near = stack(column)
    partials = mix(near, swap(near, parts), w_out, outer, groups)
    total = partials[0].astype(f32)
    for k in far_first(groups):
        total = total + between(partials[k], "tp", k, groups).astype(f32)
    return total.astype(bf16), base_state


def solution(mesh):
    in_specs = (
        P(None, "kv"),
        P("kv"),
        P("kv", "tp"),
        P("kv", "tp"),
        P("kv", "tp"),
        P("tp"),
        P("tp"),
        P("tp", "kv"),
        P("kv", "tp", None, None),
        P("kv", None, "tp"),
        P("kv", None, "tp"),
        P("kv"),
    )
    out_specs = (P(None, ("kv", "tp")), P("kv", "tp", None, None))
    step = functools.partial(body, mesh.shape["kv"], mesh.shape["tp"])
    return jax.shard_map(step, mesh=mesh, in_specs=in_specs, out_specs=out_specs, check_vma=False)
```

```python
import functools

import jax
import jax.numpy as jnp
from jax import lax
from jax.experimental import pallas as pl
from jax.experimental.pallas import tpu as pltpu
from jax.sharding import PartitionSpec as P


EPSILON = 1e-06
LANES = 128
SUBLANES = 8
PACK = 16
PAIR = 2
GROUP = 4


f32 = jnp.float32
bf16 = jnp.bfloat16
VMEM = pltpu.VMEM
WHOLE = pl.BlockSpec(memory_space=pltpu.VMEM)


def grant(mib):
    return pltpu.CompilerParams(vmem_limit_bytes=mib << 20)


def in_hbm(*arrays):
    return [pltpu.with_memory_space_constraint(a, pltpu.HBM) for a in arrays]


def round_up(n, m):
    return -(-n // m) * m


def square_rows(tokens):
    return round_up(tokens, LANES) // LANES


def coded_rows(tokens):
    return round_up(2 * square_rows(tokens), SUBLANES)


def coded(spread):
    rows = spread.shape[0]
    high = spread.astype(bf16).astype(f32)
    parts = [high, spread - high]
    pad = round_up(2 * rows, SUBLANES) - 2 * rows
    if pad:
        parts.append(jnp.zeros((pad, LANES), f32))
    return jnp.concatenate(parts, axis=0).astype(bf16)


def decoded(ref, start, rows):
    tile = ref[start : start + round_up(2 * rows, SUBLANES), :].astype(f32)
    return tile[:rows] + tile[rows : 2 * rows]


def split(x):
    high = x.astype(bf16)
    return high, (x - high.astype(f32)).astype(bf16)


def project_kernel(outer, x_hbm, gain_hbm, wq_hbm, wf_hbm, wv_hbm, *rest):
    across_ref, stay_ref, squares_ref, own_ref = rest[:4]
    ahead = rest[4 : 3 + outer]
    x_ref, gain_ref, w_ref, terms_ref, sems = rest[3 + outer :]
    tokens, features = x_ref.shape
    cols = wq_hbm.shape[1]
    blocks = cols // LANES
    local = tokens // (outer * PAIR)
    copies = [
        pltpu.make_async_copy(x_hbm, x_ref, sems.at[0]),
        pltpu.make_async_copy(gain_hbm, gain_ref, sems.at[1]),
    ]
    for j, w in enumerate((wf_hbm, wv_hbm, wq_hbm)):
        copies.append(pltpu.make_async_copy(w, w_ref.at[j], sems.at[2 + j]))
    for c in copies:
        c.start()
    copies[0].wait()
    copies[1].wait()
    wide = x_ref[...].astype(f32)
    scaled = (wide * gain_ref[...].astype(f32).reshape(1, features)).astype(bf16)
    me = lax.axis_index("kv")
    mine = lax.rem(me, PAIR)
    here = me // PAIR
    nears, fars = [], []
    for k in range(outer):
        there = target(here, k, outer) * PAIR
        nears.append(pl.ds(pl.multiple_of((there + mine) * local, PACK), local))
        fars.append(pl.ds(pl.multiple_of((there + 1 - mine) * local, PACK), local))
    for j in range(3):
        copies[2 + j].wait()
        terms = jnp.dot(scaled, w_ref[j], preferred_element_type=f32)
        for b in range(blocks):
            terms_ref[j * blocks + b] = terms[:, b * LANES : (b + 1) * LANES]
        if j == 2:
            break
        for k in range(outer):
            for b in range(j * blocks, (j + 1) * blocks):
                at = pl.ds((k * 2 * blocks + b) * local, local)
                stay_ref[at, :] = terms_ref[b, nears[k], :]
                across_ref[at, :] = terms_ref[b, fars[k], :].astype(bf16)
        if j == 0:
            squares = wide * wide
            folded = squares[:, :LANES]
            for b in range(1, features // LANES):
                folded = folded + squares[:, b * LANES : (b + 1) * LANES]
            row = jnp.sum(folded.T, axis=0, keepdims=True)
            rows = square_rows(tokens)
            spread = jnp.concatenate(
                [row[:, r * LANES : (r + 1) * LANES] for r in range(rows)], axis=0
            )
            squares_ref[...] = spread
            across_ref[outer * 2 * blocks * local :, :] = coded(spread)
    for k in range(outer):
        for b in range(blocks):
            for r, which in enumerate((nears[k], fars[k])):
                at = pl.ds((r * blocks + b) * local, local)
                piece = terms_ref[2 * blocks + b, which, :]
                if k:
                    ahead[k - 1][at, :] = piece.astype(bf16)
                else:
                    own_ref[at, :] = piece


def project(inputs, norm_gain, w_query, w_forget, w_value, outer):
    tokens, features = inputs.shape
    cols = w_query.shape[1]
    blocks = cols // LANES
    local = tokens // (outer * PAIR)
    section = 2 * blocks * local
    shapes = [
        jax.ShapeDtypeStruct((outer * section + coded_rows(tokens), LANES), bf16),
        jax.ShapeDtypeStruct((outer * section, LANES), f32),
        jax.ShapeDtypeStruct((square_rows(tokens), LANES), f32),
        jax.ShapeDtypeStruct((section, LANES), f32),
    ] + [jax.ShapeDtypeStruct((section, LANES), bf16)] * (outer - 1)
    out = pl.pallas_call(
        functools.partial(project_kernel, outer),
        out_shape=shapes,
        in_specs=[pl.BlockSpec(memory_space=pltpu.HBM)] * 5,
        out_specs=[WHOLE] * len(shapes),
        scratch_shapes=[
            VMEM((tokens, features), bf16),
            VMEM((features,), bf16),
            VMEM((3, features, cols), bf16),
            VMEM((3 * blocks, tokens, LANES), f32),
            pltpu.SemaphoreType.DMA((5,)),
        ],
        compiler_params=grant(24),
        name="project",
    )(*in_hbm(inputs, norm_gain, w_query, w_forget, w_value))
    return out[0], out[1], out[2], out[3], out[4:]


def combine_kernel(outer, after_ref, *refs):
    del after_ref
    across_ref, stay_ref, squares_ref, own_ref = refs[:4]
    ahead = refs[4 : 3 + outer]
    outs = refs[3 + outer :]
    sends, (pair_ref, kept_ref, total_ref, half_ref) = outs[: outer - 1], outs[outer - 1 :]
    rows = squares_ref.shape[0]
    section = kept_ref.shape[0]
    squares = squares_ref[...] + decoded(across_ref, outer * section, rows)
    total_ref[...] = squares
    tail = coded(squares)
    for k in range(1, outer):
        at = pl.ds(k * section, section)
        sends[k - 1][:section, :] = (stay_ref[at, :] + across_ref[at, :].astype(f32)).astype(bf16)
        sends[k - 1][section:, :] = tail
    kept_ref[...] = stay_ref[:section, :] + across_ref[:section, :].astype(f32)
    total = own_ref[...]
    for p in ahead:
        total = total + p[...].astype(f32)
    split_at = half_ref.shape[0]
    half_ref[...] = total[:split_at]
    pair_ref[...] = total[split_at:].astype(bf16)


def combine(after, across, stay, squares, own, ahead, outer):
    section = own.shape[0]
    rows = squares.shape[0]
    height = section + round_up(2 * rows, SUBLANES)
    shapes = [jax.ShapeDtypeStruct((height, LANES), bf16)] * (outer - 1) + [
        jax.ShapeDtypeStruct((section // PAIR, LANES), bf16),
        jax.ShapeDtypeStruct((section, LANES), f32),
        jax.ShapeDtypeStruct((rows, LANES), f32),
        jax.ShapeDtypeStruct((section // PAIR, LANES), f32),
    ]
    out = pl.pallas_call(
        functools.partial(combine_kernel, outer),
        out_shape=shapes,
        in_specs=[WHOLE] * (outer + 4),
        out_specs=[WHOLE] * len(shapes),
        compiler_params=grant(16),
        name="combine",
    )(after, across, stay, squares, own, *ahead)
    return out[: outer - 1], *out[outer - 1 :]


def fold_kernel(
    start, accepted_hbm, after_ref, state_hbm, gate_hbm, value_hbm, base_ref, high_ref, low_ref, *rest
):
    del after_ref
    state_ref, gate_ref, value_ref, left_ref, accepted_ref, sems, gate_sem, value_sem, accepted_sem = rest
    seqs, heads, size, _ = state_ref.shape
    proposals = gate_ref.shape[1]
    gate_copy = pltpu.make_async_copy(gate_hbm.at[pl.ds(start, seqs)], gate_ref, gate_sem)
    value_copy = pltpu.make_async_copy(value_hbm.at[pl.ds(start, seqs)], value_ref, value_sem)
    accepted_copy = pltpu.make_async_copy(accepted_hbm, accepted_ref, accepted_sem)
    accepted_copy.start()
    gate_copy.start()
    value_copy.start()
    loads = [
        pltpu.make_async_copy(state_hbm.at[start + s], state_ref.at[s], sems.at[s])
        for s in range(seqs)
    ]
    for c in loads:
        c.start()
    accepted_copy.wait()
    gate_copy.wait()
    value_copy.wait()
    each = 3 * (proposals + 1)
    depth = round_up(each, PACK)
    none = jnp.zeros((1, size), f32)
    one = jnp.ones((1, size), f32)
    fill = [none] * (depth - each)
    side = jnp.concatenate(([none] * proposals + [one]) * 3 + fill, axis=0)
    for s in range(seqs):
        taken = accepted_ref[start + s]
        gates = gate_ref[s]
        total = jnp.ones_like(gates[:1])
        weights = [None] * proposals
        for j in reversed(range(proposals)):
            use = j < taken
            gate = gates[j : j + 1]
            weights[j] = jnp.where(use, (1.0 - gate) * total, 0.0)
            total = jnp.where(use, gate * total, total)
        exact = jnp.concatenate(weights + [total], axis=0)
        first = exact.astype(bf16).astype(f32)
        second = (exact - first).astype(bf16).astype(f32)
        third = exact - first - second
        pad = [jnp.zeros((depth - each, exact.shape[1]), f32)] if depth > each else []
        left = jnp.concatenate([first, second, third] + pad, axis=0)
        left = jnp.concatenate([left[:, h * size : (h + 1) * size] for h in range(heads)], axis=0)
        left_ref[s] = left.T.astype(bf16)
    rows = lax.broadcasted_iota(jnp.int32, (heads * depth, 2 * size), 0) // depth
    for s in range(seqs):
        if s % GROUP == 0:
            for c in loads[s : s + GROUP]:
                c.wait()
        values = value_ref[s].astype(f32)
        left = left_ref[s]
        for h in range(heads):
            mine = values[:, h * size : (h + 1) * size]
            block = jnp.concatenate([mine, none] * 3 + fill, axis=0)
            block = jnp.concatenate((block, side), axis=1)
            right = jnp.where(rows == h, jnp.concatenate([block] * heads, axis=0), 0.0)
            both = jnp.dot(left, right.astype(bf16), preferred_element_type=f32)
            base = both[:, size:] * state_ref[s, h] + both[:, :size]
            base_ref[s, h] = base
            high, low = split(base)
            high_ref[s, h] = high
            low_ref[s, h] = low


def fold(start, seqs, accepted, after, prior_state, prev_forget, prev_values):
    heads, size = prior_state.shape[1:3]
    proposals, cols = prev_forget.shape[1:]
    shape = (seqs, heads, size, size)
    hbm = pl.BlockSpec(memory_space=pltpu.HBM)
    return pl.pallas_call(
        functools.partial(fold_kernel, start),
        out_shape=[
            jax.ShapeDtypeStruct(shape, f32),
            jax.ShapeDtypeStruct(shape, bf16),
            jax.ShapeDtypeStruct(shape, bf16),
        ],
        in_specs=[hbm, pl.BlockSpec(memory_space=pl.ANY)] + [hbm] * 3,
        out_specs=[WHOLE] * 3,
        scratch_shapes=[
            VMEM(shape, f32),
            VMEM((seqs, proposals, cols), f32),
            VMEM((seqs, proposals, cols), bf16),
            VMEM((seqs, size, heads * round_up(3 * (proposals + 1), PACK)), bf16),
            pltpu.SMEM(accepted.shape, jnp.int32),
            pltpu.SemaphoreType.DMA((seqs,)),
            pltpu.SemaphoreType.DMA,
            pltpu.SemaphoreType.DMA,
            pltpu.SemaphoreType.DMA,
        ],
        cost_estimate=pl.CostEstimate(
            flops=1_000_000_000, bytes_accessed=12 * prior_state.size, transcendentals=0
        ),
        compiler_params=grant(16),
        name="fold",
    )(*in_hbm(accepted), after, *in_hbm(prior_state, prev_forget, prev_values))


def store_kernel(count, after_ref, *refs):
    del after_ref
    bases, out_hbm, sems = refs[:count], refs[count], refs[count + 1]
    copies = []
    for base_ref in bases:
        for s in range(base_ref.shape[0]):
            place = len(copies)
            copies.append(
                pltpu.make_async_copy(base_ref.at[s], out_hbm.at[place], sems.at[place])
            )
    for c in copies:
        c.start()
    for c in copies:
        c.wait()


def store(after, bases):
    seqs = sum(base.shape[0] for base in bases)
    shape = (seqs, *bases[0].shape[1:])
    return pl.pallas_call(
        functools.partial(store_kernel, len(bases)),
        out_shape=jax.ShapeDtypeStruct(shape, f32),
        in_specs=[WHOLE] * (1 + len(bases)),
        out_specs=pl.BlockSpec(memory_space=pltpu.HBM),
        scratch_shapes=[pltpu.SemaphoreType.DMA((seqs,))],
        cost_estimate=pl.CostEstimate(
            flops=1_000_000_000, bytes_accessed=8 * seqs, transcendentals=0
        ),
        compiler_params=grant(8),
        name="store",
    )(after, *bases)


def recur_kernel(seqs, proposals, width, count, *refs):
    kept_ref, squares_ref, half_ref, other_ref = refs[:4]
    highs_ref, lows_ref = refs[4 : 4 + count], refs[4 + count : 4 + 2 * count]
    arrived = refs[4 + 2 * count : -5]
    floor_ref, gain_ref, out_ref, sum_ref, rows_ref = refs[-5:]
    heads, size = highs_ref[0].shape[1:3]
    local = seqs * proposals
    rows = squares_ref.shape[0]
    section = kept_ref.shape[0]
    total = kept_ref[...]
    squares = squares_ref[...]
    for p in arrived:
        total = total + p[:section, :].astype(f32)
        squares = squares + decoded(p, section, rows)
    first = half_ref[...] + other_ref[...].astype(f32)
    me = lax.axis_index("kv")
    lane = lax.broadcasted_iota(jnp.int32, (local, LANES), 1)
    token = lax.broadcasted_iota(jnp.int32, (local, LANES), 0) + me * local
    picked = jnp.zeros((local, LANES), f32)
    for r in range(rows):
        picked = jnp.where(lane + r * LANES == token, squares[r : r + 1], picked)
    column = jnp.sum(picked, axis=1, keepdims=True)
    scale = lax.rsqrt(column / width + EPSILON)
    for b in range(heads):
        sum_ref[b * local : (b + 1) * local, :] = first[b * local : (b + 1) * local] * scale
    for b in range(2 * heads):
        at = slice((heads + b) * local, (heads + b + 1) * local)
        sum_ref[at, :] = total[b * local : (b + 1) * local] * scale
    for h in range(heads):
        at = slice(h * size, (h + 1) * size)

        def take(kind, t):
            return sum_ref[pl.ds((kind * heads + h) * local + t, seqs, stride=proposals), :]

        floor = floor_ref[:, at]
        head_gain = gain_ref[:, at]
        query, forget, key, value = [], [], [], []
        for t in range(proposals):
            q = take(0, t)
            query.append(q / (1.0 + jnp.exp(-q)))
            g = floor + (1.0 - floor) / (1.0 + jnp.exp(-take(1, t)))
            forget.append(g)
            key.append(1.0 - g)
            value.append(take(2, t))
        lefts = []
        mixes = []
        for t in range(proposals):
            carried = query[t]
            mix = None
            for j in reversed(range(t + 1)):
                weight = jnp.sum(carried * key[j], axis=1, keepdims=True) * value[j]
                mix = weight if mix is None else mix + weight
                carried = carried * forget[j]
            lefts.append(carried)
            mixes.append(mix)
        highs = [x.astype(bf16).astype(f32) for x in lefts]
        lows = [x - y for x, y in zip(lefts, highs)]
        both = jnp.concatenate(highs + lows, axis=0)
        sub_all = lax.broadcasted_iota(jnp.int32, both.shape, 0) % seqs
        left = jnp.concatenate(
            [jnp.where(sub_all == s, both, 0.0).astype(bf16) for s in range(seqs)], axis=1
        )
        high = jnp.concatenate([r[:, h].reshape(-1, size) for r in highs_ref], axis=0)
        low = jnp.concatenate([r[:, h].reshape(-1, size) for r in lows_ref], axis=0)
        first = jnp.dot(left, high, preferred_element_type=f32)
        second = jnp.dot(left[:local], low, preferred_element_type=f32)
        read = first[:local] + first[local:] + second
        for t in range(proposals):
            result = read[t * seqs : (t + 1) * seqs] + mixes[t]
            mean = jnp.sum(result * result, axis=1, keepdims=True) / size
            rows_ref[pl.ds(h * local + t, seqs, stride=proposals), :] = (
                result * lax.rsqrt(mean + EPSILON) * head_gain
            )
        out_ref[:, at] = rows_ref[h * local : (h + 1) * local, :].astype(bf16)


def recur(kept, squares, half, other, highs, lows, arrived, lower_bound, head_gain, proposals, width):
    count = len(highs)
    seqs = sum(h.shape[0] for h in highs)
    heads, size = highs[0].shape[1:3]
    local = seqs * proposals
    cols = heads * size
    return pl.pallas_call(
        functools.partial(recur_kernel, seqs, proposals, width, count),
        out_shape=jax.ShapeDtypeStruct((local, cols), bf16),
        in_specs=[WHOLE] * (len(arrived) + 6 + 2 * count),
        out_specs=WHOLE,
        scratch_shapes=[VMEM((3 * heads * local, size), f32), VMEM((heads * local, size), f32)],
        compiler_params=grant(16),
        name="recur",
    )(
        kept,
        squares,
        half,
        other,
        *highs,
        *lows,
        *arrived,
        lower_bound.reshape(1, cols),
        head_gain.reshape(1, cols),
    )


def stack_kernel(count, *refs):
    pieces, out_ref = refs[:count], refs[count]
    local = pieces[0].shape[0]
    for k in range(count):
        out_ref[k * local : (k + 1) * local, :] = pieces[k][...]


def stack(pieces):
    count = len(pieces)
    local, cols = pieces[0].shape
    return pl.pallas_call(
        functools.partial(stack_kernel, count),
        out_shape=jax.ShapeDtypeStruct((count * local, cols), bf16),
        in_specs=[WHOLE] * count,
        out_specs=WHOLE,
        compiler_params=grant(8),
        name="stack",
    )(*pieces)


def mix_kernel(groups, own_ref, others_ref, near_w_ref, upper_ref, lower_ref, keep_ref, send_ref, cols_ref):
    half = groups // PAIR
    height = own_ref.shape[0] + others_ref.shape[0]
    left = jnp.concatenate((own_ref[...], others_ref[...]), axis=0)
    span = near_w_ref.shape[1] // groups
    far_w = jnp.concatenate((upper_ref[...], lower_ref[...]), axis=0)
    for side, w in enumerate((near_w_ref[...], far_w)):
        partial = jnp.dot(left, w, preferred_element_type=f32)
        for g in range(groups):
            cols_ref[side, g] = partial[:, g * span : (g + 1) * span]
    me = lax.axis_index("tp")
    mine = lax.rem(me, PAIR)
    for side in range(PAIR):
        for k in range(half):
            group = target(me // PAIR, k, half) * PAIR
            at = pl.ds((side * half + k) * height, height)
            keep_ref[at, :] = cols_ref[side, group + mine]
            send_ref[at, :] = cols_ref[side, group + 1 - mine].astype(bf16)


def mix(own, others, near_w, upper, lower, groups):
    height = own.shape[0] + others.shape[0]
    span = near_w.shape[1] // groups
    return pl.pallas_call(
        functools.partial(mix_kernel, groups),
        out_shape=[
            jax.ShapeDtypeStruct((groups * height, span), f32),
            jax.ShapeDtypeStruct((groups * height, span), bf16),
        ],
        in_specs=[WHOLE] * 5,
        out_specs=[WHOLE] * 2,
        scratch_shapes=[VMEM((PAIR, groups, height, span), f32)],
        compiler_params=grant(16),
        name="mix",
    )(own, others, near_w, upper, lower)


def join_kernel(keep_ref, other_ref, own_ref, *outs):
    height = own_ref.shape[0]
    total = keep_ref[...] + other_ref[...].astype(f32)
    own_ref[...] = total[:height]
    for i, out in enumerate(outs):
        out[...] = total[(i + 1) * height : (i + 2) * height].astype(bf16)


def join(keep, other, groups):
    height, span = keep.shape[0] // groups, keep.shape[1]
    out = pl.pallas_call(
        join_kernel,
        out_shape=[jax.ShapeDtypeStruct((height, span), f32)]
        + [jax.ShapeDtypeStruct((height, span), bf16)] * (groups - 1),
        in_specs=[WHOLE] * 2,
        out_specs=[WHOLE] * groups,
        compiler_params=grant(8),
        name="join",
    )(keep, other)
    return out[0], out[1:]


def finish_kernel(outer, groups, *refs):
    out_ref = refs[-1]
    half = groups // PAIR
    local = refs[0].shape[0] // outer
    me = lax.axis_index("kv")
    here = me // PAIR
    mine = lax.rem(me, PAIR)
    for side, pieces in ((mine, refs[:half]), (1 - mine, refs[half:groups])):
        total = pieces[0][...].astype(f32)
        for p in pieces[1:]:
            total = total + p[...].astype(f32)
        total = total.astype(bf16)
        for i, k in enumerate([0] + far_first(outer)):
            place = (origin(here, k, outer) * PAIR + side) * local
            out_ref[pl.ds(pl.multiple_of(place, PACK), local), :] = total[i * local : (i + 1) * local]


def finish(pieces, outer):
    groups = len(pieces)
    height, span = pieces[0].shape
    return pl.pallas_call(
        functools.partial(finish_kernel, outer, groups),
        out_shape=jax.ShapeDtypeStruct((PAIR * height, span), bf16),
        in_specs=[WHOLE] * groups,
        out_specs=WHOLE,
        compiler_params=grant(8),
        name="finish",
    )(*pieces)


def target(here, k, count):
    return here ^ k if count & (count - 1) == 0 else (here + k) % count


def origin(here, k, count):
    return here ^ k if count & (count - 1) == 0 else (here + count - k) % count


def far_first(count):
    return sorted(range(1, count), key=lambda k: -k)


def across_groups(x, k, groups, parts, other):
    half = groups // PAIR
    moves = []
    for s in range(parts):
        to = s - s % PAIR + (s + other) % PAIR
        for g in range(groups):
            there = target(g // PAIR, k, half) * PAIR + g % PAIR
            moves.append((s * groups + g, to * groups + there))
    return lax.ppermute(x, ("kv", "tp"), moves)


def swap(x, axis, count):
    return lax.ppermute(x, axis, [(s, s - s % PAIR + (s + 1) % PAIR) for s in range(count)])


def along(x, k, parts):
    count = parts // PAIR
    return lax.ppermute(
        x, "kv", [(s, PAIR * target(s // PAIR, k, count) + s % PAIR) for s in range(parts)]
    )


def body(
    parts,
    groups,
    inputs,
    norm_gain,
    w_query,
    w_forget,
    w_value,
    lower_bound,
    head_gain,
    w_out,
    prior_state,
    prev_forget,
    prev_values,
    accepted,
):
    width = inputs.shape[1] * parts
    outer = parts // PAIR
    order = far_first(outer)
    across, stay, squares, own, ahead = project(
        inputs, norm_gain, w_query, w_forget, w_value, outer
    )
    across = swap(across, "kv", parts)
    moved = []
    for k in order:
        moved.append(along(ahead[k - 1], k, parts))
    ahead = moved
    cut = w_out.shape[0] // 2
    upper = swap(w_out[:cut], "kv", parts)
    state = (prior_state, prev_forget, prev_values)
    seqs = prior_state.shape[0]
    early = seqs // 2
    base, high, low = fold(0, early, accepted, stay, *state)
    sends, pair, kept, squares, half = combine(
        low, across, stay, squares, own, ahead, outer
    )
    late_base, late_high, late_low = fold(early, seqs - early, accepted, pair, *state)
    arrived = []
    for k in order:
        arrived.append(along(sends[k - 1], k, parts))
    base_state = store(pair, (base, late_base))
    other = swap(pair, "kv", parts)
    lower = swap(w_out[cut:], "kv", parts)
    normed = recur(
        kept,
        squares,
        half,
        other,
        (high, late_high),
        (low, late_low),
        arrived,
        lower_bound,
        head_gain,
        prev_forget.shape[1],
        width,
    )
    column = []
    for k in order:
        column.append(along(normed, k, parts))
    near = stack(column)
    keep, send = mix(normed, near, w_out, upper, lower, groups)
    own, sends = join(keep, swap(send, "tp", groups), groups)
    half = groups // PAIR
    pieces = [own] + [None] * (groups - 1)
    for i in reversed(range(1, groups)):
        pieces[i] = across_groups(sends[i - 1], i % half, groups, parts, i // half)
    return finish(pieces, outer), base_state


def solution(mesh):
    in_specs = (
        P(None, "kv"),
        P("kv"),
        P("kv", "tp"),
        P("kv", "tp"),
        P("kv", "tp"),
        P("tp"),
        P("tp"),
        P("tp", "kv"),
        P("kv", "tp", None, None),
        P("kv", None, "tp"),
        P("kv", None, "tp"),
        P("kv"),
    )
    out_specs = (P(None, ("kv", "tp")), P("kv", "tp", None, None))
    step = functools.partial(body, mesh.shape["kv"], mesh.shape["tp"])
    step = jax.shard_map(step, mesh=mesh, in_specs=in_specs, out_specs=out_specs, check_vma=False)
    return step
```

```python
import functools

import jax
import jax.numpy as jnp
from jax import lax
from jax.experimental import pallas as pl
from jax.experimental.pallas import tpu as pltpu
from jax.sharding import PartitionSpec as P


EPSILON = 1e-06
LANES = 128
SUBLANES = 8
PACK = 16
PAIR = 2
GROUP = 4


f32 = jnp.float32
bf16 = jnp.bfloat16
VMEM = pltpu.VMEM
WHOLE = pl.BlockSpec(memory_space=pltpu.VMEM)


def grant(mib):
    return pltpu.CompilerParams(vmem_limit_bytes=mib << 20)


def in_hbm(*arrays):
    return [pltpu.with_memory_space_constraint(a, pltpu.HBM) for a in arrays]


def round_up(n, m):
    return -(-n // m) * m


def square_rows(tokens):
    return round_up(tokens, LANES) // LANES


def coded_rows(tokens):
    return round_up(2 * square_rows(tokens), SUBLANES)


def coded(spread):
    rows = spread.shape[0]
    high = spread.astype(bf16).astype(f32)
    parts = [high, spread - high]
    pad = round_up(2 * rows, SUBLANES) - 2 * rows
    if pad:
        parts.append(jnp.zeros((pad, LANES), f32))
    return jnp.concatenate(parts, axis=0).astype(bf16)


def decoded(ref, start, rows):
    tile = ref[start : start + round_up(2 * rows, SUBLANES), :].astype(f32)
    return tile[:rows] + tile[rows : 2 * rows]


def split(x):
    high = x.astype(bf16)
    return high, (x - high.astype(f32)).astype(bf16)


def project_kernel(outer, x_hbm, gain_hbm, wf_hbm, wv_hbm, *rest):
    across_ref, stay_ref, squares_ref, scaled_ref, x_ref, gain_ref, w_ref, sems = rest
    tokens, features = x_ref.shape
    cols = wf_hbm.shape[1]
    blocks = cols // LANES
    local = tokens // (outer * PAIR)
    copies = [
        pltpu.make_async_copy(x_hbm, x_ref, sems.at[0]),
        pltpu.make_async_copy(gain_hbm, gain_ref, sems.at[1]),
    ]
    for j, w in enumerate((wf_hbm, wv_hbm)):
        copies.append(pltpu.make_async_copy(w, w_ref.at[j], sems.at[2 + j]))
    for c in copies:
        c.start()
    me = lax.axis_index("kv")
    mine = lax.rem(me, PAIR)
    here = me // PAIR
    copies[0].wait()
    copies[1].wait()
    gain = gain_ref[...].astype(f32).reshape(1, features)
    for k in range(outer):
        there = target(here, k, outer) * PAIR
        for r, side in enumerate((mine, 1 - mine)):
            block = x_ref[pl.ds(pl.multiple_of((there + side) * local, PACK), local), :]
            at = pl.ds((k * PAIR + r) * local, local)
            scaled_ref[at, :] = (block.astype(f32) * gain).astype(bf16)
    wide = x_ref[...].astype(f32)
    squares = wide * wide
    folded = squares[:, :LANES]
    for b in range(1, features // LANES):
        folded = folded + squares[:, b * LANES : (b + 1) * LANES]
    row = jnp.sum(folded.T, axis=0, keepdims=True)
    spread = jnp.concatenate(
        [row[:, r * LANES : (r + 1) * LANES] for r in range(square_rows(tokens))], axis=0
    )
    squares_ref[...] = spread
    across_ref[outer * 2 * blocks * local :, :] = coded(spread)
    for j in range(2):
        copies[2 + j].wait()
        terms = jnp.dot(scaled_ref[...], w_ref[j], preferred_element_type=f32)
        for k in range(outer):
            start = k * PAIR * local
            for b in range(blocks):
                at = pl.ds((k * 2 * blocks + j * blocks + b) * local, local)
                part = terms[start : start + PAIR * local, b * LANES : (b + 1) * LANES]
                stay_ref[at, :] = part[:local]
                across_ref[at, :] = part[local:].astype(bf16)


def project(inputs, norm_gain, w_forget, w_value, outer):
    tokens, features = inputs.shape
    cols = w_forget.shape[1]
    section = 2 * cols // LANES * tokens // (outer * PAIR)
    return pl.pallas_call(
        functools.partial(project_kernel, outer),
        out_shape=[
            jax.ShapeDtypeStruct((outer * section + coded_rows(tokens), LANES), bf16),
            jax.ShapeDtypeStruct((outer * section, LANES), f32),
            jax.ShapeDtypeStruct((square_rows(tokens), LANES), f32),
            jax.ShapeDtypeStruct((tokens, features), bf16),
        ],
        in_specs=[pl.BlockSpec(memory_space=pltpu.HBM)] * 4,
        out_specs=[WHOLE] * 4,
        scratch_shapes=[
            VMEM((tokens, features), bf16),
            VMEM((features,), bf16),
            VMEM((2, features, cols), bf16),
            pltpu.SemaphoreType.DMA((4,)),
        ],
        cost_estimate=pl.CostEstimate(
            flops=2_000_000_000, bytes_accessed=4 * features * cols, transcendentals=0
        ),
        compiler_params=grant(24),
        name="project",
    )(*in_hbm(inputs, norm_gain, w_forget, w_value))


def query_kernel(outer, scaled_ref, w_ref, own_ref, *ahead):
    local = scaled_ref.shape[0] // (outer * PAIR)
    blocks = w_ref.shape[1] // LANES
    terms = jnp.dot(scaled_ref[...], w_ref[...], preferred_element_type=f32)
    for k in range(outer):
        for r in range(PAIR):
            start = (k * PAIR + r) * local
            for b in range(blocks):
                at = pl.ds((r * blocks + b) * local, local)
                part = terms[start : start + local, b * LANES : (b + 1) * LANES]
                if k:
                    ahead[k - 1][at, :] = part.astype(bf16)
                else:
                    own_ref[at, :] = part


def query(scaled, w_query, outer):
    cols = w_query.shape[1]
    section = 2 * cols // LANES * scaled.shape[0] // (outer * PAIR)
    out = pl.pallas_call(
        functools.partial(query_kernel, outer),
        out_shape=[jax.ShapeDtypeStruct((section, LANES), f32)]
        + [jax.ShapeDtypeStruct((section, LANES), bf16)] * (outer - 1),
        in_specs=[WHOLE] * 2,
        out_specs=[WHOLE] * outer,
        compiler_params=grant(16),
        name="query",
    )(scaled, w_query)
    return out[0], out[1:]


def combine_kernel(outer, after_ref, *refs):
    del after_ref
    across_ref, stay_ref, squares_ref, own_ref = refs[:4]
    ahead = refs[4 : 3 + outer]
    outs = refs[3 + outer :]
    sends, (pair_ref, kept_ref, total_ref, half_ref) = outs[: outer - 1], outs[outer - 1 :]
    rows = squares_ref.shape[0]
    section = kept_ref.shape[0]
    squares = squares_ref[...] + decoded(across_ref, outer * section, rows)
    total_ref[...] = squares
    tail = coded(squares)
    for k in range(1, outer):
        at = pl.ds(k * section, section)
        sends[k - 1][:section, :] = (stay_ref[at, :] + across_ref[at, :].astype(f32)).astype(bf16)
        sends[k - 1][section:, :] = tail
    kept_ref[...] = stay_ref[:section, :] + across_ref[:section, :].astype(f32)
    total = own_ref[...]
    for p in ahead:
        total = total + p[...].astype(f32)
    split_at = half_ref.shape[0]
    half_ref[...] = total[:split_at]
    pair_ref[...] = total[split_at:].astype(bf16)


def combine(after, across, stay, squares, own, ahead, outer):
    section = own.shape[0]
    rows = squares.shape[0]
    height = section + round_up(2 * rows, SUBLANES)
    shapes = [jax.ShapeDtypeStruct((height, LANES), bf16)] * (outer - 1) + [
        jax.ShapeDtypeStruct((section // PAIR, LANES), bf16),
        jax.ShapeDtypeStruct((section, LANES), f32),
        jax.ShapeDtypeStruct((rows, LANES), f32),
        jax.ShapeDtypeStruct((section // PAIR, LANES), f32),
    ]
    out = pl.pallas_call(
        functools.partial(combine_kernel, outer),
        out_shape=shapes,
        in_specs=[WHOLE] * (outer + 4),
        out_specs=[WHOLE] * len(shapes),
        compiler_params=grant(16),
        name="combine",
    )(after, across, stay, squares, own, *ahead)
    return out[: outer - 1], *out[outer - 1 :]


def fold_kernel(
    start, accepted_hbm, after_ref, state_hbm, gate_hbm, value_hbm, base_ref, high_ref, low_ref, *rest
):
    del after_ref
    state_ref, gate_ref, value_ref, left_ref, accepted_ref, sems, gate_sem, value_sem, accepted_sem = rest
    seqs, heads, size, _ = state_ref.shape
    proposals = gate_ref.shape[1]
    gate_copy = pltpu.make_async_copy(gate_hbm.at[pl.ds(start, seqs)], gate_ref, gate_sem)
    value_copy = pltpu.make_async_copy(value_hbm.at[pl.ds(start, seqs)], value_ref, value_sem)
    accepted_copy = pltpu.make_async_copy(accepted_hbm, accepted_ref, accepted_sem)
    accepted_copy.start()
    gate_copy.start()
    value_copy.start()
    loads = [
        pltpu.make_async_copy(state_hbm.at[start + s], state_ref.at[s], sems.at[s])
        for s in range(seqs)
    ]
    for c in loads:
        c.start()
    accepted_copy.wait()
    gate_copy.wait()
    value_copy.wait()
    each = 3 * (proposals + 1)
    depth = round_up(each, PACK)
    none = jnp.zeros((1, size), f32)
    one = jnp.ones((1, size), f32)
    fill = [none] * (depth - each)
    side = jnp.concatenate(([none] * proposals + [one]) * 3 + fill, axis=0)
    for s in range(seqs):
        taken = accepted_ref[start + s]
        gates = gate_ref[s]
        total = jnp.ones_like(gates[:1])
        weights = [None] * proposals
        for j in reversed(range(proposals)):
            use = j < taken
            gate = gates[j : j + 1]
            weights[j] = jnp.where(use, (1.0 - gate) * total, 0.0)
            total = jnp.where(use, gate * total, total)
        exact = jnp.concatenate(weights + [total], axis=0)
        first = exact.astype(bf16).astype(f32)
        second = (exact - first).astype(bf16).astype(f32)
        third = exact - first - second
        pad = [jnp.zeros((depth - each, exact.shape[1]), f32)] if depth > each else []
        left = jnp.concatenate([first, second, third] + pad, axis=0)
        left = jnp.concatenate([left[:, h * size : (h + 1) * size] for h in range(heads)], axis=0)
        left_ref[s] = left.T.astype(bf16)
    rows = lax.broadcasted_iota(jnp.int32, (heads * depth, 2 * size), 0) // depth
    for s in range(seqs):
        if s % GROUP == 0:
            for c in loads[s : s + GROUP]:
                c.wait()
        values = value_ref[s].astype(f32)
        left = left_ref[s]
        for h in range(heads):
            mine = values[:, h * size : (h + 1) * size]
            block = jnp.concatenate([mine, none] * 3 + fill, axis=0)
            block = jnp.concatenate((block, side), axis=1)
            right = jnp.where(rows == h, jnp.concatenate([block] * heads, axis=0), 0.0)
            both = jnp.dot(left, right.astype(bf16), preferred_element_type=f32)
            base = both[:, size:] * state_ref[s, h] + both[:, :size]
            base_ref[s, h] = base
            high, low = split(base)
            high_ref[s, h] = high
            low_ref[s, h] = low


def fold(start, seqs, accepted, after, prior_state, prev_forget, prev_values):
    heads, size = prior_state.shape[1:3]
    proposals, cols = prev_forget.shape[1:]
    shape = (seqs, heads, size, size)
    hbm = pl.BlockSpec(memory_space=pltpu.HBM)
    return pl.pallas_call(
        functools.partial(fold_kernel, start),
        out_shape=[
            jax.ShapeDtypeStruct(shape, f32),
            jax.ShapeDtypeStruct(shape, bf16),
            jax.ShapeDtypeStruct(shape, bf16),
        ],
        in_specs=[hbm, pl.BlockSpec(memory_space=pl.ANY)] + [hbm] * 3,
        out_specs=[WHOLE] * 3,
        scratch_shapes=[
            VMEM(shape, f32),
            VMEM((seqs, proposals, cols), f32),
            VMEM((seqs, proposals, cols), bf16),
            VMEM((seqs, size, heads * round_up(3 * (proposals + 1), PACK)), bf16),
            pltpu.SMEM(accepted.shape, jnp.int32),
            pltpu.SemaphoreType.DMA((seqs,)),
            pltpu.SemaphoreType.DMA,
            pltpu.SemaphoreType.DMA,
            pltpu.SemaphoreType.DMA,
        ],
        cost_estimate=pl.CostEstimate(
            flops=1_000_000_000, bytes_accessed=12 * prior_state.size, transcendentals=0
        ),
        compiler_params=grant(16),
        name="fold",
    )(*in_hbm(accepted), after, *in_hbm(prior_state, prev_forget, prev_values))


def store_kernel(count, after_ref, *refs):
    del after_ref
    bases, out_hbm, sems = refs[:count], refs[count], refs[count + 1]
    copies = []
    for base_ref in bases:
        for s in range(base_ref.shape[0]):
            place = len(copies)
            copies.append(
                pltpu.make_async_copy(base_ref.at[s], out_hbm.at[place], sems.at[place])
            )
    for c in copies:
        c.start()
    for c in copies:
        c.wait()


def store(after, bases):
    seqs = sum(base.shape[0] for base in bases)
    shape = (seqs, *bases[0].shape[1:])
    return pl.pallas_call(
        functools.partial(store_kernel, len(bases)),
        out_shape=jax.ShapeDtypeStruct(shape, f32),
        in_specs=[WHOLE] * (1 + len(bases)),
        out_specs=pl.BlockSpec(memory_space=pltpu.HBM),
        scratch_shapes=[pltpu.SemaphoreType.DMA((seqs,))],
        cost_estimate=pl.CostEstimate(
            flops=1_000_000_000, bytes_accessed=8 * seqs, transcendentals=0
        ),
        compiler_params=grant(8),
        name="store",
    )(after, *bases)


def recur_kernel(seqs, proposals, width, count, *refs):
    kept_ref, squares_ref, half_ref, other_ref = refs[:4]
    highs_ref, lows_ref = refs[4 : 4 + count], refs[4 + count : 4 + 2 * count]
    arrived = refs[4 + 2 * count : -5]
    floor_ref, gain_ref, out_ref, sum_ref, rows_ref = refs[-5:]
    heads, size = highs_ref[0].shape[1:3]
    local = seqs * proposals
    rows = squares_ref.shape[0]
    section = kept_ref.shape[0]
    total = kept_ref[...]
    squares = squares_ref[...]
    for p in arrived:
        total = total + p[:section, :].astype(f32)
        squares = squares + decoded(p, section, rows)
    first = half_ref[...] + other_ref[...].astype(f32)
    me = lax.axis_index("kv")
    lane = lax.broadcasted_iota(jnp.int32, (local, LANES), 1)
    token = lax.broadcasted_iota(jnp.int32, (local, LANES), 0) + me * local
    picked = jnp.zeros((local, LANES), f32)
    for r in range(rows):
        picked = jnp.where(lane + r * LANES == token, squares[r : r + 1], picked)
    column = jnp.sum(picked, axis=1, keepdims=True)
    scale = lax.rsqrt(column / width + EPSILON)
    for b in range(heads):
        sum_ref[b * local : (b + 1) * local, :] = first[b * local : (b + 1) * local] * scale
    for b in range(2 * heads):
        at = slice((heads + b) * local, (heads + b + 1) * local)
        sum_ref[at, :] = total[b * local : (b + 1) * local] * scale
    for h in range(heads):
        at = slice(h * size, (h + 1) * size)

        def take(kind, t):
            return sum_ref[pl.ds((kind * heads + h) * local + t, seqs, stride=proposals), :]

        floor = floor_ref[:, at]
        head_gain = gain_ref[:, at]
        query, forget, key, value = [], [], [], []
        for t in range(proposals):
            q = take(0, t)
            query.append(q / (1.0 + jnp.exp(-q)))
            g = floor + (1.0 - floor) / (1.0 + jnp.exp(-take(1, t)))
            forget.append(g)
            key.append(1.0 - g)
            value.append(take(2, t))
        lefts = []
        mixes = []
        for t in range(proposals):
            carried = query[t]
            mix = None
            for j in reversed(range(t + 1)):
                weight = jnp.sum(carried * key[j], axis=1, keepdims=True) * value[j]
                mix = weight if mix is None else mix + weight
                carried = carried * forget[j]
            lefts.append(carried)
            mixes.append(mix)
        highs = [x.astype(bf16).astype(f32) for x in lefts]
        lows = [x - y for x, y in zip(lefts, highs)]
        both = jnp.concatenate(highs + lows, axis=0)
        sub_all = lax.broadcasted_iota(jnp.int32, both.shape, 0) % seqs
        left = jnp.concatenate(
            [jnp.where(sub_all == s, both, 0.0).astype(bf16) for s in range(seqs)], axis=1
        )
        high = jnp.concatenate([r[:, h].reshape(-1, size) for r in highs_ref], axis=0)
        low = jnp.concatenate([r[:, h].reshape(-1, size) for r in lows_ref], axis=0)
        first = jnp.dot(left, high, preferred_element_type=f32)
        second = jnp.dot(left[:local], low, preferred_element_type=f32)
        read = first[:local] + first[local:] + second
        for t in range(proposals):
            result = read[t * seqs : (t + 1) * seqs] + mixes[t]
            mean = jnp.sum(result * result, axis=1, keepdims=True) / size
            rows_ref[pl.ds(h * local + t, seqs, stride=proposals), :] = (
                result * lax.rsqrt(mean + EPSILON) * head_gain
            )
        out_ref[:, at] = rows_ref[h * local : (h + 1) * local, :].astype(bf16)


def recur(kept, squares, half, other, highs, lows, arrived, lower_bound, head_gain, proposals, width):
    count = len(highs)
    seqs = sum(h.shape[0] for h in highs)
    heads, size = highs[0].shape[1:3]
    local = seqs * proposals
    cols = heads * size
    return pl.pallas_call(
        functools.partial(recur_kernel, seqs, proposals, width, count),
        out_shape=jax.ShapeDtypeStruct((local, cols), bf16),
        in_specs=[WHOLE] * (len(arrived) + 6 + 2 * count),
        out_specs=WHOLE,
        scratch_shapes=[VMEM((3 * heads * local, size), f32), VMEM((heads * local, size), f32)],
        compiler_params=grant(16),
        name="recur",
    )(
        kept,
        squares,
        half,
        other,
        *highs,
        *lows,
        *arrived,
        lower_bound.reshape(1, cols),
        head_gain.reshape(1, cols),
    )


def stack_kernel(count, *refs):
    pieces, out_ref = refs[:count], refs[count]
    local = pieces[0].shape[0]
    for k in range(count):
        out_ref[k * local : (k + 1) * local, :] = pieces[k][...]


def stack(pieces):
    count = len(pieces)
    local, cols = pieces[0].shape
    return pl.pallas_call(
        functools.partial(stack_kernel, count),
        out_shape=jax.ShapeDtypeStruct((count * local, cols), bf16),
        in_specs=[WHOLE] * count,
        out_specs=WHOLE,
        compiler_params=grant(8),
        name="stack",
    )(*pieces)


def mix_kernel(groups, own_ref, others_ref, near_w_ref, upper_ref, lower_ref, keep_ref, send_ref, cols_ref):
    half = groups // PAIR
    height = own_ref.shape[0] + others_ref.shape[0]
    left = jnp.concatenate((own_ref[...], others_ref[...]), axis=0)
    span = near_w_ref.shape[1] // groups
    far_w = jnp.concatenate((upper_ref[...], lower_ref[...]), axis=0)
    for side, w in enumerate((near_w_ref[...], far_w)):
        partial = jnp.dot(left, w, preferred_element_type=f32)
        for g in range(groups):
            cols_ref[side, g] = partial[:, g * span : (g + 1) * span]
    me = lax.axis_index("tp")
    mine = lax.rem(me, PAIR)
    for side in range(PAIR):
        for k in range(half):
            group = target(me // PAIR, k, half) * PAIR
            at = pl.ds((side * half + k) * height, height)
            keep_ref[at, :] = cols_ref[side, group + mine]
            send_ref[at, :] = cols_ref[side, group + 1 - mine].astype(bf16)


def mix(own, others, near_w, upper, lower, groups):
    height = own.shape[0] + others.shape[0]
    span = near_w.shape[1] // groups
    return pl.pallas_call(
        functools.partial(mix_kernel, groups),
        out_shape=[
            jax.ShapeDtypeStruct((groups * height, span), f32),
            jax.ShapeDtypeStruct((groups * height, span), bf16),
        ],
        in_specs=[WHOLE] * 5,
        out_specs=[WHOLE] * 2,
        scratch_shapes=[VMEM((PAIR, groups, height, span), f32)],
        compiler_params=grant(16),
        name="mix",
    )(own, others, near_w, upper, lower)


def join_kernel(keep_ref, other_ref, own_ref, *outs):
    height = own_ref.shape[0]
    total = keep_ref[...] + other_ref[...].astype(f32)
    own_ref[...] = total[:height]
    for i, out in enumerate(outs):
        out[...] = total[(i + 1) * height : (i + 2) * height].astype(bf16)


def join(keep, other, groups):
    height, span = keep.shape[0] // groups, keep.shape[1]
    out = pl.pallas_call(
        join_kernel,
        out_shape=[jax.ShapeDtypeStruct((height, span), f32)]
        + [jax.ShapeDtypeStruct((height, span), bf16)] * (groups - 1),
        in_specs=[WHOLE] * 2,
        out_specs=[WHOLE] * groups,
        compiler_params=grant(8),
        name="join",
    )(keep, other)
    return out[0], out[1:]


def finish_kernel(outer, groups, *refs):
    out_ref = refs[-1]
    half = groups // PAIR
    local = refs[0].shape[0] // outer
    me = lax.axis_index("kv")
    here = me // PAIR
    mine = lax.rem(me, PAIR)
    for side, pieces in ((mine, refs[:half]), (1 - mine, refs[half:groups])):
        total = pieces[0][...].astype(f32)
        for p in pieces[1:]:
            total = total + p[...].astype(f32)
        total = total.astype(bf16)
        for i, k in enumerate([0] + far_first(outer)):
            place = (origin(here, k, outer) * PAIR + side) * local
            out_ref[pl.ds(pl.multiple_of(place, PACK), local), :] = total[i * local : (i + 1) * local]


def finish(pieces, outer):
    groups = len(pieces)
    height, span = pieces[0].shape
    return pl.pallas_call(
        functools.partial(finish_kernel, outer, groups),
        out_shape=jax.ShapeDtypeStruct((PAIR * height, span), bf16),
        in_specs=[WHOLE] * groups,
        out_specs=WHOLE,
        compiler_params=grant(8),
        name="finish",
    )(*pieces)


def target(here, k, count):
    return here ^ k if count & (count - 1) == 0 else (here + k) % count


def origin(here, k, count):
    return here ^ k if count & (count - 1) == 0 else (here + count - k) % count


def far_first(count):
    return sorted(range(1, count), key=lambda k: -k)


def across_groups(x, k, groups, parts, other):
    half = groups // PAIR
    moves = []
    for s in range(parts):
        to = s - s % PAIR + (s + other) % PAIR
        for g in range(groups):
            there = target(g // PAIR, k, half) * PAIR + g % PAIR
            moves.append((s * groups + g, to * groups + there))
    return lax.ppermute(x, ("kv", "tp"), moves)


def swap(x, axis, count):
    return lax.ppermute(x, axis, [(s, s - s % PAIR + (s + 1) % PAIR) for s in range(count)])


def along(x, k, parts):
    count = parts // PAIR
    return lax.ppermute(
        x, "kv", [(s, PAIR * target(s // PAIR, k, count) + s % PAIR) for s in range(parts)]
    )


def body(
    parts,
    groups,
    inputs,
    norm_gain,
    w_query,
    w_forget,
    w_value,
    lower_bound,
    head_gain,
    w_out,
    prior_state,
    prev_forget,
    prev_values,
    accepted,
):
    width = inputs.shape[1] * parts
    outer = parts // PAIR
    order = far_first(outer)
    across, stay, squares, scaled = project(inputs, norm_gain, w_forget, w_value, outer)
    across = swap(across, "kv", parts)
    own, ahead = query(scaled, w_query, outer)
    moved = []
    for k in order:
        moved.append(along(ahead[k - 1], k, parts))
    ahead = moved
    cut = w_out.shape[0] // 2
    upper = swap(w_out[:cut], "kv", parts)
    state = (prior_state, prev_forget, prev_values)
    seqs = prior_state.shape[0]
    early = seqs // 2
    base, high, low = fold(0, early, accepted, stay, *state)
    sends, pair, kept, squares, half = combine(
        low, across, stay, squares, own, ahead, outer
    )
    late_base, late_high, late_low = fold(early, seqs - early, accepted, pair, *state)
    arrived = []
    for k in order:
        arrived.append(along(sends[k - 1], k, parts))
    base_state = store(pair, (base, late_base))
    other = swap(pair, "kv", parts)
    lower = swap(w_out[cut:], "kv", parts)
    normed = recur(
        kept,
        squares,
        half,
        other,
        (high, late_high),
        (low, late_low),
        arrived,
        lower_bound,
        head_gain,
        prev_forget.shape[1],
        width,
    )
    column = []
    for k in order:
        column.append(along(normed, k, parts))
    near = stack(column)
    keep, send = mix(normed, near, w_out, upper, lower, groups)
    own, sends = join(keep, swap(send, "tp", groups), groups)
    half = groups // PAIR
    pieces = [own] + [None] * (groups - 1)
    for i in reversed(range(1, groups)):
        pieces[i] = across_groups(sends[i - 1], i % half, groups, parts, i // half)
    return finish(pieces, outer), base_state


def solution(mesh):
    in_specs = (
        P(None, "kv"),
        P("kv"),
        P("kv", "tp"),
        P("kv", "tp"),
        P("kv", "tp"),
        P("tp"),
        P("tp"),
        P("tp", "kv"),
        P("kv", "tp", None, None),
        P("kv", None, "tp"),
        P("kv", None, "tp"),
        P("kv"),
    )
    out_specs = (P(None, ("kv", "tp")), P("kv", "tp", None, None))
    step = functools.partial(body, mesh.shape["kv"], mesh.shape["tp"])
    step = jax.shard_map(step, mesh=mesh, in_specs=in_specs, out_specs=out_specs, check_vma=False)
    return step
```

```python
import functools

import jax
import jax.numpy as jnp
from jax import lax
from jax.experimental import pallas as pl
from jax.experimental.pallas import tpu as pltpu
from jax.sharding import PartitionSpec as P


EPSILON = 1e-06
LANES = 128
SUBLANES = 8
PACK = 16
PAIR = 2
GROUP = 4


f32 = jnp.float32
bf16 = jnp.bfloat16
VMEM = pltpu.VMEM
WHOLE = pl.BlockSpec(memory_space=pltpu.VMEM)


def grant(mib):
    return pltpu.CompilerParams(vmem_limit_bytes=mib << 20)


def in_hbm(*arrays):
    return [pltpu.with_memory_space_constraint(a, pltpu.HBM) for a in arrays]


def round_up(n, m):
    return -(-n // m) * m


def square_rows(tokens):
    return round_up(tokens, LANES) // LANES


def coded_rows(tokens):
    return round_up(2 * square_rows(tokens), SUBLANES)


def coded(spread):
    rows = spread.shape[0]
    high = spread.astype(bf16).astype(f32)
    parts = [high, spread - high]
    pad = round_up(2 * rows, SUBLANES) - 2 * rows
    if pad:
        parts.append(jnp.zeros((pad, LANES), f32))
    return jnp.concatenate(parts, axis=0).astype(bf16)


def decoded(ref, start, rows):
    tile = ref[start : start + round_up(2 * rows, SUBLANES), :].astype(f32)
    return tile[:rows] + tile[rows : 2 * rows]


def split(x):
    high = x.astype(bf16)
    return high, (x - high.astype(f32)).astype(bf16)


def project_kernel(outer, x_hbm, gain_hbm, wf_hbm, wv_hbm, *rest):
    across_ref, stay_ref, squares_ref, scaled_ref, x_ref, gain_ref, w_ref, sems = rest
    tokens, features = x_ref.shape
    cols = wf_hbm.shape[1]
    blocks = cols // LANES
    local = tokens // (outer * PAIR)
    copies = [
        pltpu.make_async_copy(x_hbm, x_ref, sems.at[0]),
        pltpu.make_async_copy(gain_hbm, gain_ref, sems.at[1]),
    ]
    for j, w in enumerate((wf_hbm, wv_hbm)):
        copies.append(pltpu.make_async_copy(w, w_ref.at[j], sems.at[2 + j]))
    for c in copies:
        c.start()
    me = lax.axis_index("kv")
    mine = lax.rem(me, PAIR)
    here = me // PAIR
    copies[0].wait()
    copies[1].wait()
    gain = gain_ref[...].astype(f32).reshape(1, features)
    for k in range(outer):
        there = target(here, k, outer) * PAIR
        for r, side in enumerate((mine, 1 - mine)):
            block = x_ref[pl.ds(pl.multiple_of((there + side) * local, PACK), local), :]
            at = pl.ds((k * PAIR + r) * local, local)
            scaled_ref[at, :] = (block.astype(f32) * gain).astype(bf16)
    wide = x_ref[...].astype(f32)
    squares = wide * wide
    folded = squares[:, :LANES]
    for b in range(1, features // LANES):
        folded = folded + squares[:, b * LANES : (b + 1) * LANES]
    row = jnp.sum(folded.T, axis=0, keepdims=True)
    spread = jnp.concatenate(
        [row[:, r * LANES : (r + 1) * LANES] for r in range(square_rows(tokens))], axis=0
    )
    squares_ref[...] = spread
    across_ref[outer * 2 * blocks * local :, :] = coded(spread)
    for j in range(2):
        copies[2 + j].wait()
        terms = jnp.dot(scaled_ref[...], w_ref[j], preferred_element_type=f32)
        for k in range(outer):
            start = k * PAIR * local
            for b in range(blocks):
                at = pl.ds((k * 2 * blocks + j * blocks + b) * local, local)
                part = terms[start : start + PAIR * local, b * LANES : (b + 1) * LANES]
                stay_ref[at, :] = part[:local]
                across_ref[at, :] = part[local:].astype(bf16)


def project(inputs, norm_gain, w_forget, w_value, outer):
    tokens, features = inputs.shape
    cols = w_forget.shape[1]
    section = 2 * cols // LANES * tokens // (outer * PAIR)
    return pl.pallas_call(
        functools.partial(project_kernel, outer),
        out_shape=[
            jax.ShapeDtypeStruct((outer * section + coded_rows(tokens), LANES), bf16),
            jax.ShapeDtypeStruct((outer * section, LANES), f32),
            jax.ShapeDtypeStruct((square_rows(tokens), LANES), f32),
            jax.ShapeDtypeStruct((tokens, features), bf16),
        ],
        in_specs=[pl.BlockSpec(memory_space=pltpu.HBM)] * 4,
        out_specs=[WHOLE] * 4,
        scratch_shapes=[
            VMEM((tokens, features), bf16),
            VMEM((features,), bf16),
            VMEM((2, features, cols), bf16),
            pltpu.SemaphoreType.DMA((4,)),
        ],
        cost_estimate=pl.CostEstimate(
            flops=2_000_000_000, bytes_accessed=4 * features * cols, transcendentals=0
        ),
        compiler_params=grant(24),
        name="project",
    )(*in_hbm(inputs, norm_gain, w_forget, w_value))


def query_kernel(outer, scaled_ref, w_ref, own_ref, *ahead):
    local = scaled_ref.shape[0] // (outer * PAIR)
    blocks = w_ref.shape[1] // LANES
    terms = jnp.dot(scaled_ref[...], w_ref[...], preferred_element_type=f32)
    for k in range(outer):
        for r in range(PAIR):
            start = (k * PAIR + r) * local
            for b in range(blocks):
                at = pl.ds((r * blocks + b) * local, local)
                part = terms[start : start + local, b * LANES : (b + 1) * LANES]
                if k:
                    ahead[k - 1][at, :] = part.astype(bf16)
                else:
                    own_ref[at, :] = part


def query(scaled, w_query, outer):
    cols = w_query.shape[1]
    section = 2 * cols // LANES * scaled.shape[0] // (outer * PAIR)
    out = pl.pallas_call(
        functools.partial(query_kernel, outer),
        out_shape=[jax.ShapeDtypeStruct((section, LANES), f32)]
        + [jax.ShapeDtypeStruct((section, LANES), bf16)] * (outer - 1),
        in_specs=[WHOLE] * 2,
        out_specs=[WHOLE] * outer,
        compiler_params=grant(16),
        name="query",
    )(scaled, w_query)
    return out[0], out[1:]


def combine_kernel(outer, after_ref, *refs):
    del after_ref
    across_ref, stay_ref, squares_ref, own_ref = refs[:4]
    ahead = refs[4 : 3 + outer]
    outs = refs[3 + outer :]
    sends, (pair_ref, kept_ref, total_ref, half_ref) = outs[: outer - 1], outs[outer - 1 :]
    rows = squares_ref.shape[0]
    section = kept_ref.shape[0]
    squares = squares_ref[...] + decoded(across_ref, outer * section, rows)
    total_ref[...] = squares
    tail = coded(squares)
    for k in range(1, outer):
        at = pl.ds(k * section, section)
        sends[k - 1][:section, :] = (stay_ref[at, :] + across_ref[at, :].astype(f32)).astype(bf16)
        sends[k - 1][section:, :] = tail
    kept_ref[...] = stay_ref[:section, :] + across_ref[:section, :].astype(f32)
    total = own_ref[...]
    for p in ahead:
        total = total + p[...].astype(f32)
    split_at = half_ref.shape[0]
    half_ref[...] = total[:split_at]
    pair_ref[...] = total[split_at:].astype(bf16)


def combine(after, across, stay, squares, own, ahead, outer):
    section = own.shape[0]
    rows = squares.shape[0]
    height = section + round_up(2 * rows, SUBLANES)
    shapes = [jax.ShapeDtypeStruct((height, LANES), bf16)] * (outer - 1) + [
        jax.ShapeDtypeStruct((section // PAIR, LANES), bf16),
        jax.ShapeDtypeStruct((section, LANES), f32),
        jax.ShapeDtypeStruct((rows, LANES), f32),
        jax.ShapeDtypeStruct((section // PAIR, LANES), f32),
    ]
    out = pl.pallas_call(
        functools.partial(combine_kernel, outer),
        out_shape=shapes,
        in_specs=[WHOLE] * (outer + 4),
        out_specs=[WHOLE] * len(shapes),
        compiler_params=grant(16),
        name="combine",
    )(after, across, stay, squares, own, *ahead)
    return out[: outer - 1], *out[outer - 1 :]


def fold_kernel(
    start, accepted_hbm, after_ref, state_hbm, gate_hbm, value_hbm, base_ref, high_ref, low_ref, *rest
):
    del after_ref
    state_ref, gate_ref, value_ref, left_ref, accepted_ref, sems, gate_sem, value_sem, accepted_sem = rest
    seqs, heads, size, _ = state_ref.shape
    proposals = gate_ref.shape[1]
    gate_copy = pltpu.make_async_copy(gate_hbm.at[pl.ds(start, seqs)], gate_ref, gate_sem)
    value_copy = pltpu.make_async_copy(value_hbm.at[pl.ds(start, seqs)], value_ref, value_sem)
    accepted_copy = pltpu.make_async_copy(accepted_hbm, accepted_ref, accepted_sem)
    accepted_copy.start()
    gate_copy.start()
    value_copy.start()
    loads = [
        pltpu.make_async_copy(state_hbm.at[start + s], state_ref.at[s], sems.at[s])
        for s in range(seqs)
    ]
    for c in loads:
        c.start()
    accepted_copy.wait()
    gate_copy.wait()
    value_copy.wait()
    each = 3 * (proposals + 1)
    depth = round_up(each, PACK)
    none = jnp.zeros((1, size), f32)
    one = jnp.ones((1, size), f32)
    fill = [none] * (depth - each)
    side = jnp.concatenate(([none] * proposals + [one]) * 3 + fill, axis=0)
    for s in range(seqs):
        taken = accepted_ref[start + s]
        gates = gate_ref[s]
        total = jnp.ones_like(gates[:1])
        weights = [None] * proposals
        for j in reversed(range(proposals)):
            use = j < taken
            gate = gates[j : j + 1]
            weights[j] = jnp.where(use, (1.0 - gate) * total, 0.0)
            total = jnp.where(use, gate * total, total)
        exact = jnp.concatenate(weights + [total], axis=0)
        first = exact.astype(bf16).astype(f32)
        second = (exact - first).astype(bf16).astype(f32)
        third = exact - first - second
        pad = [jnp.zeros((depth - each, exact.shape[1]), f32)] if depth > each else []
        left = jnp.concatenate([first, second, third] + pad, axis=0)
        left = jnp.concatenate([left[:, h * size : (h + 1) * size] for h in range(heads)], axis=0)
        left_ref[s] = left.T.astype(bf16)
    rows = lax.broadcasted_iota(jnp.int32, (heads * depth, 2 * size), 0) // depth
    for s in range(seqs):
        if s % GROUP == 0:
            for c in loads[s : s + GROUP]:
                c.wait()
        values = value_ref[s].astype(f32)
        left = left_ref[s]
        for h in range(heads):
            mine = values[:, h * size : (h + 1) * size]
            block = jnp.concatenate([mine, none] * 3 + fill, axis=0)
            block = jnp.concatenate((block, side), axis=1)
            right = jnp.where(rows == h, jnp.concatenate([block] * heads, axis=0), 0.0)
            both = jnp.dot(left, right.astype(bf16), preferred_element_type=f32)
            base = both[:, size:] * state_ref[s, h] + both[:, :size]
            base_ref[s, h] = base
            high, low = split(base)
            high_ref[s, h] = high
            low_ref[s, h] = low


def fold(start, seqs, accepted, after, prior_state, prev_forget, prev_values):
    heads, size = prior_state.shape[1:3]
    proposals, cols = prev_forget.shape[1:]
    shape = (seqs, heads, size, size)
    hbm = pl.BlockSpec(memory_space=pltpu.HBM)
    return pl.pallas_call(
        functools.partial(fold_kernel, start),
        out_shape=[
            jax.ShapeDtypeStruct(shape, f32),
            jax.ShapeDtypeStruct(shape, bf16),
            jax.ShapeDtypeStruct(shape, bf16),
        ],
        in_specs=[hbm, pl.BlockSpec(memory_space=pl.ANY)] + [hbm] * 3,
        out_specs=[WHOLE] * 3,
        scratch_shapes=[
            VMEM(shape, f32),
            VMEM((seqs, proposals, cols), f32),
            VMEM((seqs, proposals, cols), bf16),
            VMEM((seqs, size, heads * round_up(3 * (proposals + 1), PACK)), bf16),
            pltpu.SMEM(accepted.shape, jnp.int32),
            pltpu.SemaphoreType.DMA((seqs,)),
            pltpu.SemaphoreType.DMA,
            pltpu.SemaphoreType.DMA,
            pltpu.SemaphoreType.DMA,
        ],
        cost_estimate=pl.CostEstimate(
            flops=1_000_000_000, bytes_accessed=12 * prior_state.size, transcendentals=0
        ),
        compiler_params=grant(16),
        name="fold",
    )(*in_hbm(accepted), after, *in_hbm(prior_state, prev_forget, prev_values))


def store_kernel(count, after_ref, *refs):
    del after_ref
    bases, out_hbm, sems = refs[:count], refs[count], refs[count + 1]
    copies = []
    for base_ref in bases:
        for s in range(base_ref.shape[0]):
            place = len(copies)
            copies.append(
                pltpu.make_async_copy(base_ref.at[s], out_hbm.at[place], sems.at[place])
            )
    for c in copies:
        c.start()
    for c in copies:
        c.wait()


def store(after, bases):
    seqs = sum(base.shape[0] for base in bases)
    shape = (seqs, *bases[0].shape[1:])
    return pl.pallas_call(
        functools.partial(store_kernel, len(bases)),
        out_shape=jax.ShapeDtypeStruct(shape, f32),
        in_specs=[WHOLE] * (1 + len(bases)),
        out_specs=pl.BlockSpec(memory_space=pltpu.HBM),
        scratch_shapes=[pltpu.SemaphoreType.DMA((seqs,))],
        cost_estimate=pl.CostEstimate(
            flops=1_000_000_000, bytes_accessed=8 * seqs, transcendentals=0
        ),
        compiler_params=grant(8),
        name="store",
    )(after, *bases)


def recur_kernel(seqs, proposals, width, count, *refs):
    kept_ref, squares_ref, half_ref, other_ref = refs[:4]
    highs_ref, lows_ref = refs[4 : 4 + count], refs[4 + count : 4 + 2 * count]
    arrived = refs[4 + 2 * count : -5]
    floor_ref, gain_ref, out_ref, sum_ref, rows_ref = refs[-5:]
    heads, size = highs_ref[0].shape[1:3]
    local = seqs * proposals
    rows = squares_ref.shape[0]
    section = kept_ref.shape[0]
    total = kept_ref[...]
    squares = squares_ref[...]
    for p in arrived:
        total = total + p[:section, :].astype(f32)
        squares = squares + decoded(p, section, rows)
    first = half_ref[...] + other_ref[...].astype(f32)
    me = lax.axis_index("kv")
    lane = lax.broadcasted_iota(jnp.int32, (local, LANES), 1)
    token = lax.broadcasted_iota(jnp.int32, (local, LANES), 0) + me * local
    picked = jnp.zeros((local, LANES), f32)
    for r in range(rows):
        picked = jnp.where(lane + r * LANES == token, squares[r : r + 1], picked)
    column = jnp.sum(picked, axis=1, keepdims=True)
    scale = lax.rsqrt(column / width + EPSILON)
    for b in range(heads):
        sum_ref[b * local : (b + 1) * local, :] = first[b * local : (b + 1) * local] * scale
    for b in range(2 * heads):
        at = slice((heads + b) * local, (heads + b + 1) * local)
        sum_ref[at, :] = total[b * local : (b + 1) * local] * scale
    for h in range(heads):
        at = slice(h * size, (h + 1) * size)

        def take(kind, t):
            return sum_ref[pl.ds((kind * heads + h) * local + t, seqs, stride=proposals), :]

        floor = floor_ref[:, at]
        head_gain = gain_ref[:, at]
        query, forget, key, value = [], [], [], []
        for t in range(proposals):
            q = take(0, t)
            query.append(q / (1.0 + jnp.exp(-q)))
            g = floor + (1.0 - floor) / (1.0 + jnp.exp(-take(1, t)))
            forget.append(g)
            key.append(1.0 - g)
            value.append(take(2, t))
        lefts = []
        mixes = []
        for t in range(proposals):
            carried = query[t]
            mix = None
            for j in reversed(range(t + 1)):
                weight = jnp.sum(carried * key[j], axis=1, keepdims=True) * value[j]
                mix = weight if mix is None else mix + weight
                carried = carried * forget[j]
            lefts.append(carried)
            mixes.append(mix)
        highs = [x.astype(bf16).astype(f32) for x in lefts]
        lows = [x - y for x, y in zip(lefts, highs)]
        both = jnp.concatenate(highs + lows, axis=0)
        sub_all = lax.broadcasted_iota(jnp.int32, both.shape, 0) % seqs
        left = jnp.concatenate(
            [jnp.where(sub_all == s, both, 0.0).astype(bf16) for s in range(seqs)], axis=1
        )
        high = jnp.concatenate([r[:, h].reshape(-1, size) for r in highs_ref], axis=0)
        low = jnp.concatenate([r[:, h].reshape(-1, size) for r in lows_ref], axis=0)
        first = jnp.dot(left, high, preferred_element_type=f32)
        second = jnp.dot(left[:local], low, preferred_element_type=f32)
        read = first[:local] + first[local:] + second
        for t in range(proposals):
            result = read[t * seqs : (t + 1) * seqs] + mixes[t]
            mean = jnp.sum(result * result, axis=1, keepdims=True) / size
            rows_ref[pl.ds(h * local + t, seqs, stride=proposals), :] = (
                result * lax.rsqrt(mean + EPSILON) * head_gain
            )
        out_ref[:, at] = rows_ref[h * local : (h + 1) * local, :].astype(bf16)


def recur(kept, squares, half, other, highs, lows, arrived, lower_bound, head_gain, proposals, width):
    count = len(highs)
    seqs = sum(h.shape[0] for h in highs)
    heads, size = highs[0].shape[1:3]
    local = seqs * proposals
    cols = heads * size
    return pl.pallas_call(
        functools.partial(recur_kernel, seqs, proposals, width, count),
        out_shape=jax.ShapeDtypeStruct((local, cols), bf16),
        in_specs=[WHOLE] * (len(arrived) + 6 + 2 * count),
        out_specs=WHOLE,
        scratch_shapes=[VMEM((3 * heads * local, size), f32), VMEM((heads * local, size), f32)],
        compiler_params=grant(16),
        name="recur",
    )(
        kept,
        squares,
        half,
        other,
        *highs,
        *lows,
        *arrived,
        lower_bound.reshape(1, cols),
        head_gain.reshape(1, cols),
    )


def stack_kernel(count, *refs):
    pieces, out_ref = refs[:count], refs[count]
    local = pieces[0].shape[0]
    for k in range(count):
        out_ref[k * local : (k + 1) * local, :] = pieces[k][...]


def stack(pieces):
    count = len(pieces)
    local, cols = pieces[0].shape
    return pl.pallas_call(
        functools.partial(stack_kernel, count),
        out_shape=jax.ShapeDtypeStruct((count * local, cols), bf16),
        in_specs=[WHOLE] * count,
        out_specs=WHOLE,
        compiler_params=grant(8),
        name="stack",
    )(*pieces)


def mix_kernel(groups, own_ref, others_ref, near_w_ref, upper_ref, lower_ref, keep_ref, send_ref, cols_ref):
    half = groups // PAIR
    height = own_ref.shape[0] + others_ref.shape[0]
    left = jnp.concatenate((own_ref[...], others_ref[...]), axis=0)
    span = near_w_ref.shape[1] // groups
    far_w = jnp.concatenate((upper_ref[...], lower_ref[...]), axis=0)
    for side, w in enumerate((near_w_ref[...], far_w)):
        partial = jnp.dot(left, w, preferred_element_type=f32)
        for g in range(groups):
            cols_ref[side, g] = partial[:, g * span : (g + 1) * span]
    me = lax.axis_index("tp")
    mine = lax.rem(me, PAIR)
    for side in range(PAIR):
        for k in range(half):
            group = target(me // PAIR, k, half) * PAIR
            at = pl.ds((side * half + k) * height, height)
            member = 1 - mine if side or k else mine
            keep_ref[at, :] = cols_ref[side, group + member]
            send_ref[at, :] = cols_ref[side, group + 1 - member].astype(bf16)


def mix(own, others, near_w, upper, lower, groups):
    height = own.shape[0] + others.shape[0]
    span = near_w.shape[1] // groups
    return pl.pallas_call(
        functools.partial(mix_kernel, groups),
        out_shape=[
            jax.ShapeDtypeStruct((groups * height, span), f32),
            jax.ShapeDtypeStruct((groups * height, span), bf16),
        ],
        in_specs=[WHOLE] * 5,
        out_specs=[WHOLE] * 2,
        scratch_shapes=[VMEM((PAIR, groups, height, span), f32)],
        compiler_params=grant(16),
        name="mix",
    )(own, others, near_w, upper, lower)


def join_kernel(keep_ref, other_ref, own_ref, *outs):
    height = own_ref.shape[0]
    total = keep_ref[...] + other_ref[...].astype(f32)
    own_ref[...] = total[:height]
    for i, out in enumerate(outs):
        out[...] = total[(i + 1) * height : (i + 2) * height].astype(bf16)


def join(keep, other, groups):
    height, span = keep.shape[0] // groups, keep.shape[1]
    out = pl.pallas_call(
        join_kernel,
        out_shape=[jax.ShapeDtypeStruct((height, span), f32)]
        + [jax.ShapeDtypeStruct((height, span), bf16)] * (groups - 1),
        in_specs=[WHOLE] * 2,
        out_specs=[WHOLE] * groups,
        compiler_params=grant(8),
        name="join",
    )(keep, other)
    return out[0], out[1:]


def finish_kernel(outer, groups, *refs):
    out_ref = refs[-1]
    half = groups // PAIR
    local = refs[0].shape[0] // outer
    me = lax.axis_index("kv")
    here = me // PAIR
    mine = lax.rem(me, PAIR)
    for side, pieces in ((mine, refs[:half]), (1 - mine, refs[half:groups])):
        total = pieces[0][...].astype(f32)
        for p in pieces[1:]:
            total = total + p[...].astype(f32)
        total = total.astype(bf16)
        for i, k in enumerate([0] + far_first(outer)):
            place = (origin(here, k, outer) * PAIR + side) * local
            out_ref[pl.ds(pl.multiple_of(place, PACK), local), :] = total[i * local : (i + 1) * local]


def finish(pieces, outer):
    groups = len(pieces)
    height, span = pieces[0].shape
    return pl.pallas_call(
        functools.partial(finish_kernel, outer, groups),
        out_shape=jax.ShapeDtypeStruct((PAIR * height, span), bf16),
        in_specs=[WHOLE] * groups,
        out_specs=WHOLE,
        compiler_params=grant(8),
        name="finish",
    )(*pieces)


def target(here, k, count):
    return here ^ k if count & (count - 1) == 0 else (here + k) % count


def origin(here, k, count):
    return here ^ k if count & (count - 1) == 0 else (here + count - k) % count


def far_first(count):
    return sorted(range(1, count), key=lambda k: -k)


def cross(x, parts, groups, pair=0, outer=0, half=0, member=1):
    moves = []
    for s in range(parts):
        to = target(s // PAIR, outer, parts // PAIR) * PAIR + (s + pair) % PAIR
        for g in range(groups):
            there = target(g // PAIR, half, groups // PAIR) * PAIR + (g + member) % PAIR
            moves.append((s * groups + g, to * groups + there))
    return lax.ppermute(x, ("kv", "tp"), moves)


def swap(x, axis, count):
    return lax.ppermute(x, axis, [(s, s - s % PAIR + (s + 1) % PAIR) for s in range(count)])


def along(x, k, parts):
    count = parts // PAIR
    return lax.ppermute(
        x, "kv", [(s, PAIR * target(s // PAIR, k, count) + s % PAIR) for s in range(parts)]
    )


def body(
    parts,
    groups,
    inputs,
    norm_gain,
    w_query,
    w_forget,
    w_value,
    lower_bound,
    head_gain,
    w_out,
    prior_state,
    prev_forget,
    prev_values,
    accepted,
):
    width = inputs.shape[1] * parts
    outer = parts // PAIR
    order = far_first(outer)
    across, stay, squares, scaled = project(inputs, norm_gain, w_forget, w_value, outer)
    across = swap(across, "kv", parts)
    own, ahead = query(scaled, w_query, outer)
    moved = []
    for k in order:
        moved.append(along(ahead[k - 1], k, parts))
    ahead = moved
    cut = w_out.shape[0] // 2
    upper = swap(w_out[:cut], "kv", parts)
    state = (prior_state, prev_forget, prev_values)
    seqs = prior_state.shape[0]
    early = seqs // 2
    base, high, low = fold(0, early, accepted, stay, *state)
    sends, pair, kept, squares, half = combine(
        low, across, stay, squares, own, ahead, outer
    )
    late_base, late_high, late_low = fold(early, seqs - early, accepted, pair, *state)
    arrived = []
    for k in order:
        arrived.append(along(sends[k - 1], k, parts))
    base_state = store(pair, (base, late_base))
    other = swap(pair, "kv", parts)
    lower = swap(w_out[cut:], "kv", parts)
    normed = recur(
        kept,
        squares,
        half,
        other,
        (high, late_high),
        (low, late_low),
        arrived,
        lower_bound,
        head_gain,
        prev_forget.shape[1],
        width,
    )
    column = []
    for k in order:
        column.append(along(normed, k, parts))
    near = stack(column)
    keep, send = mix(normed, near, w_out, upper, lower, groups)
    own, sends = join(keep, swap(send, "tp", groups), groups)
    half = groups // PAIR
    pieces = [own] + [None] * (groups - 1)
    for i in reversed(range(1, groups)):
        pieces[i] = cross(sends[i - 1], parts, groups, pair=i // half, half=i % half)
    return finish(pieces, outer), base_state


def solution(mesh):
    in_specs = (
        P(None, "kv"),
        P("kv"),
        P("kv", "tp"),
        P("kv", "tp"),
        P("kv", "tp"),
        P("tp"),
        P("tp"),
        P("tp", "kv"),
        P("kv", "tp", None, None),
        P("kv", None, "tp"),
        P("kv", None, "tp"),
        P("kv"),
    )
    out_specs = (P(None, ("kv", "tp")), P("kv", "tp", None, None))
    step = functools.partial(body, mesh.shape["kv"], mesh.shape["tp"])
    step = jax.shard_map(step, mesh=mesh, in_specs=in_specs, out_specs=out_specs, check_vma=False)
    return step
```

```python
import functools

import jax
import jax.numpy as jnp
from jax import lax
from jax.experimental import pallas as pl
from jax.experimental.pallas import tpu as pltpu
from jax.sharding import PartitionSpec as P


EPSILON = 1e-06
LANES = 128
SUBLANES = 8
PACK = 16
PAIR = 2
GROUP = 4


f32 = jnp.float32
bf16 = jnp.bfloat16
VMEM = pltpu.VMEM
WHOLE = pl.BlockSpec(memory_space=pltpu.VMEM)


def grant(mib):
    return pltpu.CompilerParams(vmem_limit_bytes=mib << 20)


def in_hbm(*arrays):
    return [pltpu.with_memory_space_constraint(a, pltpu.HBM) for a in arrays]


def round_up(n, m):
    return -(-n // m) * m


def square_rows(tokens):
    return round_up(tokens, LANES) // LANES


def coded_rows(tokens):
    return round_up(2 * square_rows(tokens), SUBLANES)


def coded(spread):
    rows = spread.shape[0]
    high = spread.astype(bf16).astype(f32)
    parts = [high, spread - high]
    pad = round_up(2 * rows, SUBLANES) - 2 * rows
    if pad:
        parts.append(jnp.zeros((pad, LANES), f32))
    return jnp.concatenate(parts, axis=0).astype(bf16)


def decoded(ref, start, rows):
    tile = ref[start : start + round_up(2 * rows, SUBLANES), :].astype(f32)
    return tile[:rows] + tile[rows : 2 * rows]


def split(x):
    high = x.astype(bf16)
    return high, (x - high.astype(f32)).astype(bf16)


def project_kernel(outer, x_hbm, gain_hbm, wf_hbm, wv_hbm, *rest):
    across_ref, stay_ref, squares_ref, scaled_ref, x_ref, gain_ref, w_ref, sems = rest
    tokens, features = x_ref.shape
    cols = wf_hbm.shape[1]
    blocks = cols // LANES
    local = tokens // (outer * PAIR)
    copies = [
        pltpu.make_async_copy(x_hbm, x_ref, sems.at[0]),
        pltpu.make_async_copy(gain_hbm, gain_ref, sems.at[1]),
    ]
    for j, w in enumerate((wf_hbm, wv_hbm)):
        copies.append(pltpu.make_async_copy(w, w_ref.at[j], sems.at[2 + j]))
    for c in copies:
        c.start()
    me = lax.axis_index("kv")
    mine = lax.rem(me, PAIR)
    here = me // PAIR
    copies[0].wait()
    copies[1].wait()
    gain = gain_ref[...].astype(f32).reshape(1, features)
    for k in range(outer):
        there = target(here, k, outer) * PAIR
        for r, side in enumerate((mine, 1 - mine)):
            block = x_ref[pl.ds(pl.multiple_of((there + side) * local, PACK), local), :]
            at = pl.ds((k * PAIR + r) * local, local)
            scaled_ref[at, :] = (block.astype(f32) * gain).astype(bf16)
    wide = x_ref[...].astype(f32)
    squares = wide * wide
    folded = squares[:, :LANES]
    for b in range(1, features // LANES):
        folded = folded + squares[:, b * LANES : (b + 1) * LANES]
    row = jnp.sum(folded.T, axis=0, keepdims=True)
    spread = jnp.concatenate(
        [row[:, r * LANES : (r + 1) * LANES] for r in range(square_rows(tokens))], axis=0
    )
    squares_ref[...] = spread
    across_ref[outer * 2 * blocks * local :, :] = coded(spread)
    for j in range(2):
        copies[2 + j].wait()
        terms = jnp.dot(scaled_ref[...], w_ref[j], preferred_element_type=f32)
        for k in range(outer):
            start = k * PAIR * local
            for b in range(blocks):
                at = pl.ds((k * 2 * blocks + j * blocks + b) * local, local)
                part = terms[start : start + PAIR * local, b * LANES : (b + 1) * LANES]
                stay_ref[at, :] = part[:local]
                across_ref[at, :] = part[local:].astype(bf16)


def project(inputs, norm_gain, w_forget, w_value, outer):
    tokens, features = inputs.shape
    cols = w_forget.shape[1]
    section = 2 * cols // LANES * tokens // (outer * PAIR)
    return pl.pallas_call(
        functools.partial(project_kernel, outer),
        out_shape=[
            jax.ShapeDtypeStruct((outer * section + coded_rows(tokens), LANES), bf16),
            jax.ShapeDtypeStruct((outer * section, LANES), f32),
            jax.ShapeDtypeStruct((square_rows(tokens), LANES), f32),
            jax.ShapeDtypeStruct((tokens, features), bf16),
        ],
        in_specs=[pl.BlockSpec(memory_space=pltpu.HBM)] * 4,
        out_specs=[WHOLE] * 4,
        scratch_shapes=[
            VMEM((tokens, features), bf16),
            VMEM((features,), bf16),
            VMEM((2, features, cols), bf16),
            pltpu.SemaphoreType.DMA((4,)),
        ],
        cost_estimate=pl.CostEstimate(
            flops=2_000_000_000, bytes_accessed=4 * features * cols, transcendentals=0
        ),
        compiler_params=grant(24),
        name="project",
    )(*in_hbm(inputs, norm_gain, w_forget, w_value))


def query_kernel(outer, scaled_ref, w_ref, own_ref, *ahead):
    local = scaled_ref.shape[0] // (outer * PAIR)
    blocks = w_ref.shape[1] // LANES
    terms = jnp.dot(scaled_ref[...], w_ref[...], preferred_element_type=f32)
    for k in range(outer):
        for r in range(PAIR):
            start = (k * PAIR + r) * local
            for b in range(blocks):
                at = pl.ds((r * blocks + b) * local, local)
                part = terms[start : start + local, b * LANES : (b + 1) * LANES]
                if k:
                    ahead[k - 1][at, :] = part.astype(bf16)
                else:
                    own_ref[at, :] = part


def query(scaled, w_query, outer):
    cols = w_query.shape[1]
    section = 2 * cols // LANES * scaled.shape[0] // (outer * PAIR)
    out = pl.pallas_call(
        functools.partial(query_kernel, outer),
        out_shape=[jax.ShapeDtypeStruct((section, LANES), f32)]
        + [jax.ShapeDtypeStruct((section, LANES), bf16)] * (outer - 1),
        in_specs=[WHOLE] * 2,
        out_specs=[WHOLE] * outer,
        compiler_params=grant(16),
        name="query",
    )(scaled, w_query)
    return out[0], out[1:]


def combine_kernel(outer, after_ref, *refs):
    del after_ref
    across_ref, stay_ref, squares_ref, own_ref = refs[:4]
    ahead = refs[4 : 3 + outer]
    outs = refs[3 + outer :]
    sends, (pair_ref, kept_ref, total_ref, half_ref) = outs[: outer - 1], outs[outer - 1 :]
    rows = squares_ref.shape[0]
    section = kept_ref.shape[0]
    squares = squares_ref[...] + decoded(across_ref, outer * section, rows)
    total_ref[...] = squares
    tail = coded(squares)
    for k in range(1, outer):
        at = pl.ds(k * section, section)
        sends[k - 1][:section, :] = (stay_ref[at, :] + across_ref[at, :].astype(f32)).astype(bf16)
        sends[k - 1][section:, :] = tail
    kept_ref[...] = stay_ref[:section, :] + across_ref[:section, :].astype(f32)
    total = own_ref[...]
    for p in ahead:
        total = total + p[...].astype(f32)
    split_at = half_ref.shape[0]
    half_ref[...] = total[:split_at]
    pair_ref[...] = total[split_at:].astype(bf16)


def combine(after, across, stay, squares, own, ahead, outer):
    section = own.shape[0]
    rows = squares.shape[0]
    height = section + round_up(2 * rows, SUBLANES)
    shapes = [jax.ShapeDtypeStruct((height, LANES), bf16)] * (outer - 1) + [
        jax.ShapeDtypeStruct((section // PAIR, LANES), bf16),
        jax.ShapeDtypeStruct((section, LANES), f32),
        jax.ShapeDtypeStruct((rows, LANES), f32),
        jax.ShapeDtypeStruct((section // PAIR, LANES), f32),
    ]
    out = pl.pallas_call(
        functools.partial(combine_kernel, outer),
        out_shape=shapes,
        in_specs=[WHOLE] * (outer + 4),
        out_specs=[WHOLE] * len(shapes),
        compiler_params=grant(16),
        name="combine",
    )(after, across, stay, squares, own, *ahead)
    return out[: outer - 1], *out[outer - 1 :]


def fold_kernel(
    start, accepted_hbm, after_ref, state_hbm, gate_hbm, value_hbm, base_ref, high_ref, low_ref, *rest
):
    del after_ref
    state_ref, gate_ref, value_ref, left_ref, accepted_ref, sems, gate_sem, value_sem, accepted_sem = rest
    seqs, heads, size, _ = state_ref.shape
    proposals = gate_ref.shape[1]
    gate_copy = pltpu.make_async_copy(gate_hbm.at[pl.ds(start, seqs)], gate_ref, gate_sem)
    value_copy = pltpu.make_async_copy(value_hbm.at[pl.ds(start, seqs)], value_ref, value_sem)
    accepted_copy = pltpu.make_async_copy(accepted_hbm, accepted_ref, accepted_sem)
    accepted_copy.start()
    gate_copy.start()
    value_copy.start()
    loads = [
        pltpu.make_async_copy(state_hbm.at[start + s], state_ref.at[s], sems.at[s])
        for s in range(seqs)
    ]
    for c in loads:
        c.start()
    accepted_copy.wait()
    gate_copy.wait()
    value_copy.wait()
    each = 3 * (proposals + 1)
    depth = round_up(each, PACK)
    none = jnp.zeros((1, size), f32)
    one = jnp.ones((1, size), f32)
    fill = [none] * (depth - each)
    side = jnp.concatenate(([none] * proposals + [one]) * 3 + fill, axis=0)
    for s in range(seqs):
        taken = accepted_ref[start + s]
        gates = gate_ref[s]
        total = jnp.ones_like(gates[:1])
        weights = [None] * proposals
        for j in reversed(range(proposals)):
            use = j < taken
            gate = gates[j : j + 1]
            weights[j] = jnp.where(use, (1.0 - gate) * total, 0.0)
            total = jnp.where(use, gate * total, total)
        exact = jnp.concatenate(weights + [total], axis=0)
        first = exact.astype(bf16).astype(f32)
        second = (exact - first).astype(bf16).astype(f32)
        third = exact - first - second
        pad = [jnp.zeros((depth - each, exact.shape[1]), f32)] if depth > each else []
        left = jnp.concatenate([first, second, third] + pad, axis=0)
        left = jnp.concatenate([left[:, h * size : (h + 1) * size] for h in range(heads)], axis=0)
        left_ref[s] = left.T.astype(bf16)
    rows = lax.broadcasted_iota(jnp.int32, (heads * depth, 2 * size), 0) // depth
    for s in range(seqs):
        if s % GROUP == 0:
            for c in loads[s : s + GROUP]:
                c.wait()
        values = value_ref[s].astype(f32)
        left = left_ref[s]
        for h in range(heads):
            mine = values[:, h * size : (h + 1) * size]
            block = jnp.concatenate([mine, none] * 3 + fill, axis=0)
            block = jnp.concatenate((block, side), axis=1)
            right = jnp.where(rows == h, jnp.concatenate([block] * heads, axis=0), 0.0)
            both = jnp.dot(left, right.astype(bf16), preferred_element_type=f32)
            base = both[:, size:] * state_ref[s, h] + both[:, :size]
            base_ref[s, h] = base
            high, low = split(base)
            high_ref[s, h] = high
            low_ref[s, h] = low


def fold(start, seqs, accepted, after, prior_state, prev_forget, prev_values):
    heads, size = prior_state.shape[1:3]
    proposals, cols = prev_forget.shape[1:]
    shape = (seqs, heads, size, size)
    hbm = pl.BlockSpec(memory_space=pltpu.HBM)
    return pl.pallas_call(
        functools.partial(fold_kernel, start),
        out_shape=[
            jax.ShapeDtypeStruct(shape, f32),
            jax.ShapeDtypeStruct(shape, bf16),
            jax.ShapeDtypeStruct(shape, bf16),
        ],
        in_specs=[hbm, pl.BlockSpec(memory_space=pl.ANY)] + [hbm] * 3,
        out_specs=[WHOLE] * 3,
        scratch_shapes=[
            VMEM(shape, f32),
            VMEM((seqs, proposals, cols), f32),
            VMEM((seqs, proposals, cols), bf16),
            VMEM((seqs, size, heads * round_up(3 * (proposals + 1), PACK)), bf16),
            pltpu.SMEM(accepted.shape, jnp.int32),
            pltpu.SemaphoreType.DMA((seqs,)),
            pltpu.SemaphoreType.DMA,
            pltpu.SemaphoreType.DMA,
            pltpu.SemaphoreType.DMA,
        ],
        cost_estimate=pl.CostEstimate(
            flops=1_000_000_000, bytes_accessed=12 * prior_state.size, transcendentals=0
        ),
        compiler_params=grant(16),
        name="fold",
    )(*in_hbm(accepted), after, *in_hbm(prior_state, prev_forget, prev_values))


def store_kernel(count, after_ref, *refs):
    del after_ref
    bases, out_hbm, sems = refs[:count], refs[count], refs[count + 1]
    copies = []
    for base_ref in bases:
        for s in range(base_ref.shape[0]):
            place = len(copies)
            copies.append(
                pltpu.make_async_copy(base_ref.at[s], out_hbm.at[place], sems.at[place])
            )
    for c in copies:
        c.start()
    for c in copies:
        c.wait()


def store(after, bases):
    seqs = sum(base.shape[0] for base in bases)
    shape = (seqs, *bases[0].shape[1:])
    return pl.pallas_call(
        functools.partial(store_kernel, len(bases)),
        out_shape=jax.ShapeDtypeStruct(shape, f32),
        in_specs=[WHOLE] * (1 + len(bases)),
        out_specs=pl.BlockSpec(memory_space=pltpu.HBM),
        scratch_shapes=[pltpu.SemaphoreType.DMA((seqs,))],
        cost_estimate=pl.CostEstimate(
            flops=1_000_000_000, bytes_accessed=8 * seqs, transcendentals=0
        ),
        compiler_params=grant(8),
        name="store",
    )(after, *bases)


def recur_kernel(seqs, proposals, width, count, *refs):
    kept_ref, squares_ref, half_ref, other_ref = refs[:4]
    highs_ref, lows_ref = refs[4 : 4 + count], refs[4 + count : 4 + 2 * count]
    arrived = refs[4 + 2 * count : -5]
    floor_ref, gain_ref, out_ref, sum_ref, rows_ref = refs[-5:]
    heads, size = highs_ref[0].shape[1:3]
    local = seqs * proposals
    rows = squares_ref.shape[0]
    section = kept_ref.shape[0]
    total = kept_ref[...]
    squares = squares_ref[...]
    for p in arrived:
        total = total + p[:section, :].astype(f32)
        squares = squares + decoded(p, section, rows)
    first = half_ref[...] + other_ref[...].astype(f32)
    me = lax.axis_index("kv")
    lane = lax.broadcasted_iota(jnp.int32, (local, LANES), 1)
    token = lax.broadcasted_iota(jnp.int32, (local, LANES), 0) + me * local
    picked = jnp.zeros((local, LANES), f32)
    for r in range(rows):
        picked = jnp.where(lane + r * LANES == token, squares[r : r + 1], picked)
    column = jnp.sum(picked, axis=1, keepdims=True)
    scale = lax.rsqrt(column / width + EPSILON)
    for b in range(heads):
        sum_ref[b * local : (b + 1) * local, :] = first[b * local : (b + 1) * local] * scale
    for b in range(2 * heads):
        at = slice((heads + b) * local, (heads + b + 1) * local)
        sum_ref[at, :] = total[b * local : (b + 1) * local] * scale
    for h in range(heads):
        at = slice(h * size, (h + 1) * size)

        def take(kind, t):
            return sum_ref[pl.ds((kind * heads + h) * local + t, seqs, stride=proposals), :]

        floor = floor_ref[:, at]
        head_gain = gain_ref[:, at]
        query, forget, key, value = [], [], [], []
        for t in range(proposals):
            q = take(0, t)
            query.append(q / (1.0 + jnp.exp(-q)))
            g = floor + (1.0 - floor) / (1.0 + jnp.exp(-take(1, t)))
            forget.append(g)
            key.append(1.0 - g)
            value.append(take(2, t))
        lefts = []
        mixes = []
        for t in range(proposals):
            carried = query[t]
            mix = None
            for j in reversed(range(t + 1)):
                weight = jnp.sum(carried * key[j], axis=1, keepdims=True) * value[j]
                mix = weight if mix is None else mix + weight
                carried = carried * forget[j]
            lefts.append(carried)
            mixes.append(mix)
        highs = [x.astype(bf16).astype(f32) for x in lefts]
        lows = [x - y for x, y in zip(lefts, highs)]
        both = jnp.concatenate(highs + lows, axis=0)
        sub_all = lax.broadcasted_iota(jnp.int32, both.shape, 0) % seqs
        left = jnp.concatenate(
            [jnp.where(sub_all == s, both, 0.0).astype(bf16) for s in range(seqs)], axis=1
        )
        high = jnp.concatenate([r[:, h].reshape(-1, size) for r in highs_ref], axis=0)
        low = jnp.concatenate([r[:, h].reshape(-1, size) for r in lows_ref], axis=0)
        first = jnp.dot(left, high, preferred_element_type=f32)
        second = jnp.dot(left[:local], low, preferred_element_type=f32)
        read = first[:local] + first[local:] + second
        for t in range(proposals):
            result = read[t * seqs : (t + 1) * seqs] + mixes[t]
            mean = jnp.sum(result * result, axis=1, keepdims=True) / size
            rows_ref[pl.ds(h * local + t, seqs, stride=proposals), :] = (
                result * lax.rsqrt(mean + EPSILON) * head_gain
            )
        out_ref[:, at] = rows_ref[h * local : (h + 1) * local, :].astype(bf16)


def recur(kept, squares, half, other, highs, lows, arrived, lower_bound, head_gain, proposals, width):
    count = len(highs)
    seqs = sum(h.shape[0] for h in highs)
    heads, size = highs[0].shape[1:3]
    local = seqs * proposals
    cols = heads * size
    return pl.pallas_call(
        functools.partial(recur_kernel, seqs, proposals, width, count),
        out_shape=jax.ShapeDtypeStruct((local, cols), bf16),
        in_specs=[WHOLE] * (len(arrived) + 6 + 2 * count),
        out_specs=WHOLE,
        scratch_shapes=[VMEM((3 * heads * local, size), f32), VMEM((heads * local, size), f32)],
        compiler_params=grant(16),
        name="recur",
    )(
        kept,
        squares,
        half,
        other,
        *highs,
        *lows,
        *arrived,
        lower_bound.reshape(1, cols),
        head_gain.reshape(1, cols),
    )


def stack_kernel(count, *refs):
    pieces, out_ref = refs[:count], refs[count]
    local = pieces[0].shape[0]
    for k in range(count):
        out_ref[k * local : (k + 1) * local, :] = pieces[k][...]


def stack(pieces):
    count = len(pieces)
    local, cols = pieces[0].shape
    return pl.pallas_call(
        functools.partial(stack_kernel, count),
        out_shape=jax.ShapeDtypeStruct((count * local, cols), bf16),
        in_specs=[WHOLE] * count,
        out_specs=WHOLE,
        compiler_params=grant(8),
        name="stack",
    )(*pieces)


def mix_kernel(groups, own_ref, others_ref, near_w_ref, upper_ref, lower_ref, keep_ref, send_ref, cols_ref):
    half = groups // PAIR
    height = own_ref.shape[0] + others_ref.shape[0]
    left = jnp.concatenate((own_ref[...], others_ref[...]), axis=0)
    span = near_w_ref.shape[1] // groups
    far_w = jnp.concatenate((upper_ref[...], lower_ref[...]), axis=0)
    for side, w in enumerate((near_w_ref[...], far_w)):
        partial = jnp.dot(left, w, preferred_element_type=f32)
        for g in range(groups):
            cols_ref[side, g] = partial[:, g * span : (g + 1) * span]
    me = lax.axis_index("tp")
    mine = lax.rem(me, PAIR)
    for side in range(PAIR):
        for k in range(half):
            group = target(me // PAIR, k, half) * PAIR
            at = pl.ds((side * half + k) * height, height)
            member = 1 - mine if side or k else mine
            keep_ref[at, :] = cols_ref[side, group + member]
            send_ref[at, :] = cols_ref[side, group + 1 - member].astype(bf16)


def mix(own, others, near_w, upper, lower, groups):
    height = own.shape[0] + others.shape[0]
    span = near_w.shape[1] // groups
    return pl.pallas_call(
        functools.partial(mix_kernel, groups),
        out_shape=[
            jax.ShapeDtypeStruct((groups * height, span), f32),
            jax.ShapeDtypeStruct((groups * height, span), bf16),
        ],
        in_specs=[WHOLE] * 5,
        out_specs=[WHOLE] * 2,
        scratch_shapes=[VMEM((PAIR, groups, height, span), f32)],
        compiler_params=grant(16),
        name="mix",
    )(own, others, near_w, upper, lower)


def join_kernel(keep_ref, other_ref, own_ref, *outs):
    height = own_ref.shape[0]
    total = keep_ref[...] + other_ref[...].astype(f32)
    own_ref[...] = total[:height]
    for i, out in enumerate(outs):
        out[...] = total[(i + 1) * height : (i + 2) * height].astype(bf16)


def join(keep, other, groups):
    height, span = keep.shape[0] // groups, keep.shape[1]
    out = pl.pallas_call(
        join_kernel,
        out_shape=[jax.ShapeDtypeStruct((height, span), f32)]
        + [jax.ShapeDtypeStruct((height, span), bf16)] * (groups - 1),
        in_specs=[WHOLE] * 2,
        out_specs=[WHOLE] * groups,
        compiler_params=grant(8),
        name="join",
    )(keep, other)
    return out[0], out[1:]


def finish_kernel(outer, groups, *refs):
    out_ref = refs[-1]
    half = groups // PAIR
    local = refs[0].shape[0] // outer
    me = lax.axis_index("kv")
    here = me // PAIR
    mine = lax.rem(me, PAIR)
    for side, pieces in ((mine, refs[:half]), (1 - mine, refs[half:groups])):
        total = pieces[0][...].astype(f32)
        for p in pieces[1:]:
            total = total + p[...].astype(f32)
        total = total.astype(bf16)
        for i, k in enumerate([0] + far_first(outer)):
            place = (origin(here, k, outer) * PAIR + side) * local
            out_ref[pl.ds(pl.multiple_of(place, PACK), local), :] = total[i * local : (i + 1) * local]


def finish(pieces, outer):
    groups = len(pieces)
    height, span = pieces[0].shape
    return pl.pallas_call(
        functools.partial(finish_kernel, outer, groups),
        out_shape=jax.ShapeDtypeStruct((PAIR * height, span), bf16),
        in_specs=[WHOLE] * groups,
        out_specs=WHOLE,
        compiler_params=grant(8),
        name="finish",
    )(*pieces)


def target(here, k, count):
    return here ^ k if count & (count - 1) == 0 else (here + k) % count


def origin(here, k, count):
    return here ^ k if count & (count - 1) == 0 else (here + count - k) % count


def far_first(count):
    return sorted(range(1, count), key=lambda k: -k)


def cross(x, parts, groups, pair=0, outer=0, half=0, member=1):
    moves = []
    for s in range(parts):
        to = target(s // PAIR, outer, parts // PAIR) * PAIR + (s + pair) % PAIR
        for g in range(groups):
            there = target(g // PAIR, half, groups // PAIR) * PAIR + (g + member) % PAIR
            moves.append((s * groups + g, to * groups + there))
    return lax.ppermute(x, ("kv", "tp"), moves)


def swap(x, axis, count):
    return lax.ppermute(x, axis, [(s, s - s % PAIR + (s + 1) % PAIR) for s in range(count)])


def along(x, k, parts):
    count = parts // PAIR
    return lax.ppermute(
        x, "kv", [(s, PAIR * target(s // PAIR, k, count) + s % PAIR) for s in range(parts)]
    )


def body(
    parts,
    groups,
    inputs,
    norm_gain,
    w_query,
    w_forget,
    w_value,
    lower_bound,
    head_gain,
    w_out,
    prior_state,
    prev_forget,
    prev_values,
    accepted,
):
    width = inputs.shape[1] * parts
    outer = parts // PAIR
    order = far_first(outer)
    across, stay, squares, scaled = project(inputs, norm_gain, w_forget, w_value, outer)
    across = swap(across, "kv", parts)
    own, ahead = query(scaled, w_query, outer)
    moved = []
    for k in order:
        moved.append(along(ahead[k - 1], k, parts))
    ahead = moved
    cut = w_out.shape[0] // 2
    upper = cross(w_out[:cut], parts, groups, pair=1)
    aside = swap(w_out, "tp", groups)
    state = (prior_state, prev_forget, prev_values)
    seqs = prior_state.shape[0]
    early = seqs // 2
    base, high, low = fold(0, early, accepted, stay, *state)
    sends, pair, kept, squares, half = combine(
        low, across, stay, squares, own, ahead, outer
    )
    late_base, late_high, late_low = fold(early, seqs - early, accepted, pair, *state)
    arrived = []
    for k in order:
        arrived.append(along(sends[k - 1], k, parts))
    base_state = store(pair, (base, late_base))
    other = swap(pair, "kv", parts)
    lower = cross(w_out[cut:], parts, groups, pair=1)
    normed = recur(
        kept,
        squares,
        half,
        other,
        (high, late_high),
        (low, late_low),
        arrived,
        lower_bound,
        head_gain,
        prev_forget.shape[1],
        width,
    )
    column = []
    for k in order:
        column.append(cross(normed, parts, groups, outer=k))
    beside = swap(normed, "tp", groups)
    near = stack(column)
    keep, send = mix(beside, near, aside, upper, lower, groups)
    own, sends = join(keep, swap(send, "tp", groups), groups)
    half = groups // PAIR
    pieces = [own] + [None] * (groups - 1)
    for i in reversed(range(1, groups)):
        pieces[i] = cross(sends[i - 1], parts, groups, pair=i // half, half=i % half)
    return finish(pieces, outer), base_state


def solution(mesh):
    in_specs = (
        P(None, "kv"),
        P("kv"),
        P("kv", "tp"),
        P("kv", "tp"),
        P("kv", "tp"),
        P("tp"),
        P("tp"),
        P("tp", "kv"),
        P("kv", "tp", None, None),
        P("kv", None, "tp"),
        P("kv", None, "tp"),
        P("kv"),
    )
    out_specs = (P(None, ("kv", "tp")), P("kv", "tp", None, None))
    step = functools.partial(body, mesh.shape["kv"], mesh.shape["tp"])
    step = jax.shard_map(step, mesh=mesh, in_specs=in_specs, out_specs=out_specs, check_vma=False)
    return step
```
